256 devices in a mesh: ep: 64 (over z, y, core), tp: 4 (over x).
Axes of the slice: x: 4, y: 4, z: 8, core: 2. Of those that a mesh axis runs over, the one named last changes fastest.
Arguments:
- tokens: bfloat16 [16384, 1024], P('ep'), may hold values from -6 to 6
- cotangent: bfloat16 [16384, 1024], P('ep'), may hold values from -1.5 to 1.5
- routing: int32 [16384, 2], P('ep'), may hold values from 0 to 127, all different within a row; in each aligned block of 256 rows (0 to 255, 256 to 511, ...) at most 12 rows name the same one
- gate_weights: float32 [16384, 2], P('ep'), may hold values from 0.1 to 0.9
- gate_proj: bfloat16 [128, 1024, 512], P('ep', None, 'tp'), may hold values from -0.1875 to 0.1875
- up_proj: bfloat16 [128, 1024, 512], P('ep', None, 'tp'), may hold values from -0.1875 to 0.1875
- down_proj: bfloat16 [128, 512, 1024], P('ep', 'tp'), may hold values from -0.25 to 0.25
Outputs:
- tokens_grad: bfloat16 [16384, 1024], P('ep')
- gates_grad: float32 [16384, 2], P('ep')
- gate_proj_grad: float32 [128, 1024, 512], P('ep', None, 'tp')
- up_proj_grad: float32 [128, 1024, 512], P('ep', None, 'tp')
- down_proj_grad: float32 [128, 512, 1024], P('ep', 'tp')
The draws below stay inside these ranges and needn't reach their ends.
Inputs may be any that keep to these rules, and one draw needn't show every extreme that they name: `routing`: each row names 2 different experts; every expert is named by some row; within each aligned block of 256 rows (the tokens of one index of ep) no expert is named by more than 12 rows, a bound that some block reaches.
All inputs are finite; a program needn't handle non-finite values.
Results may differ from the reference program's by a relative error of at most 0.0015.
Values may be sent and summed in bfloat16 or wider, within the bound.
No kernel may reach another device: no remote copies, remote signals or barrier semaphores. Data moves between devices by JAX's collectives and lax.ppermute only.
A program may use at most 128 MiB of HBM per device.

```python
import math
import jax
import jax.numpy as jnp
import numpy as np
from jax import lax

D = 1024
FF = 512
TOP = 2
TOK_DEV = 256
EXPERTS = 128
TOKENS = 16384
CAP = 12
N_EP = 64


def steps_of(own_key, shape, split, least, high):
    factor_of = 1.0
    for axis_at, parts in split:
        heights = jax.random.uniform(jax.random.fold_in(jax.random.fold_in(own_key, 6), axis_at), (parts,), jnp.float32, least / len(split), high / len(split))
        factor_of = factor_of * jnp.repeat(jnp.exp(heights), shape[axis_at] // parts).reshape((-1,) + (1,) * (len(shape) - 1 - axis_at))
    return factor_of


def shared_out(own_key, own, number, rows, number_of, top, reach, slope):
    sequence = jax.random.permutation(own_key, number_of)
    heavy_load, common = shares(number_of, rows * top, reach, slope, True), shares(number_of, rows * top, reach, slope, False)
    places = jnp.arange(number_of)

    def named(tallies, rotation):
        used = int((tallies > 0).sum())
        fixed = max(1, used // 4)
        moved = fixed + (places - fixed + rotation * (used - fixed)) % max(1, number_of - fixed)
        return jnp.zeros((number_of,), jnp.int32).at[sequence[jnp.where(places < fixed, places, moved)]].set(jnp.asarray(tallies, jnp.int32))

    tallies = jnp.where(number % 4 == 0, named(heavy_load, number // 4), named(common, number - number // 4 - 1))
    mixed = jax.random.permutation(jax.random.fold_in(own, 3), number_of)
    giver, sink = mixed[0:number_of // 2 * 2:2], mixed[1:number_of // 2 * 2:2]
    slack = jnp.minimum(tallies[giver] - 1, reach - tallies[sink]) // 2
    slack = jnp.where((giver == sequence[0]) | (sink == sequence[0]) | (tallies[sink] == 0), 0, jnp.maximum(slack, 0))
    moved = jax.random.randint(jax.random.fold_in(own, 4), (number_of // 2,), 0, 1 << 20) % (slack + 1)
    tallies = tallies.at[giver].add(-moved).at[sink].add(moved)
    labels = jnp.searchsorted(jnp.cumsum(tallies), jnp.arange(rows * top), side="right").astype(jnp.int32)
    listing = labels.reshape(top, rows).T
    listing = listing[jax.random.permutation(jax.random.fold_in(own, 1), rows)]
    rotation = jax.random.randint(jax.random.fold_in(own, 2), (rows, 1), 0, top)
    return jnp.take_along_axis(listing, (jnp.arange(top)[None, :] + rotation) % top, axis=1)


def shares(amount, total, limit, skew, full):
    portions = [(1 << 20) // math.isqrt(rank ** skew) + 1 for rank in range(1, amount + 1)]
    largest = limit if full else min(limit, max(-(-total // amount), total * portions[0] // sum(portions)))
    least = 1 if total - largest >= amount - 1 else 0
    counts, surplus = [largest] + [least] * (amount - 1), total - largest - least * (amount - 1)
    while surplus > 0:
        free = [i for i in range(1, amount) if counts[i] < largest] or [i for i in range(1, amount) if counts[i] < limit]
        pool, left = sum([portions[i] for i in free]), surplus
        for i in free:
            more = min(limit - counts[i], max(1, left * portions[i] // pool), surplus)
            counts[i] = counts[i] + more
            surplus = surplus - more
    return np.array(counts)


def gaussian(own_key, dims, scale, reach, shards=(), kind=jnp.bfloat16):
    loudness = steps_of(own_key, dims, shards, -0.22, 0.18) if shards else 1.0
    entries = jax.random.normal(own_key, dims, jnp.float32) * scale * loudness
    return jnp.minimum(jnp.maximum(entries, -reach), reach).astype(kind)


def setup_inputs(seed: int = 0) -> dict:
    streams_of = jax.random.split(jax.random.key(seed), 8)
    tokens = gaussian(streams_of[0], (TOKENS, D), 1.0, 6.0, ((0, 64),))
    cotangent = gaussian(streams_of[1], (TOKENS, D), 0.25, 1.5, ((0, 64),))
    routing_keys = jax.random.split(jax.random.fold_in(streams_of[2], 1), TOKENS // TOK_DEV)
    routing_turns = jax.random.permutation(jax.random.fold_in(streams_of[2], 3), TOKENS // TOK_DEV)
    routing = jax.vmap(lambda own, number: shared_out(jax.random.fold_in(streams_of[2], 2), own, number, TOK_DEV, EXPERTS, TOP, CAP, 2))(routing_keys, routing_turns).reshape((TOKENS, TOP))
    gate_weights = jnp.clip(0.1 + 0.79999997 * jax.random.uniform(streams_of[3], (TOKENS, TOP), jnp.float32) ** steps_of(streams_of[3], (TOKENS, TOP), ((0, 64),), -0.2, 0.2), 0.1, 0.9)
    gate_proj = gaussian(streams_of[4], (EXPERTS, D, FF), D ** -0.5, 0.1875, ((0, 64), (2, 4)))
    up_proj = gaussian(streams_of[5], (EXPERTS, D, FF), D ** -0.5, 0.1875, ((0, 64), (2, 4)))
    down_proj = gaussian(streams_of[6], (EXPERTS, FF, D), FF ** -0.5, 0.25, ((0, 64), (1, 4)))
    return dict(tokens=tokens, cotangent=cotangent, routing=routing, gate_weights=gate_weights, gate_proj=gate_proj, up_proj=up_proj, down_proj=down_proj)


def expert_pass(expert_rows, scaled, gate_matrix, up_matrix, down_matrix):
    gate_pre = jnp.dot(expert_rows, gate_matrix, preferred_element_type=jnp.float32).astype(jnp.bfloat16)
    up_pre = jnp.dot(expert_rows, up_matrix, preferred_element_type=jnp.float32).astype(jnp.bfloat16)
    gate_pre, up_pre = lax.optimization_barrier((gate_pre, up_pre))
    hidden_grad = jnp.dot(scaled, down_matrix.T, preferred_element_type=jnp.float32)
    gate_wide = gate_pre.astype(jnp.float32)
    up_wide = up_pre.astype(jnp.float32)
    sigmoid_gate = jax.nn.sigmoid(gate_wide)
    activated = gate_wide * sigmoid_gate
    hidden = activated * up_wide
    product = jnp.sum(hidden_grad * hidden, axis=-1)
    gate_pre_grad = (hidden_grad * up_wide * sigmoid_gate * (1.0 + gate_wide * (1.0 - sigmoid_gate))).astype(jnp.bfloat16)
    up_pre_grad = (hidden_grad * activated).astype(jnp.bfloat16)
    input_grad = jnp.dot(gate_pre_grad, gate_matrix.T, preferred_element_type=jnp.float32)
    input_grad = input_grad + jnp.dot(up_pre_grad, up_matrix.T, preferred_element_type=jnp.float32)
    down_grad = jnp.dot(hidden.astype(jnp.bfloat16).T, scaled, preferred_element_type=jnp.float32)
    gate_grad = jnp.dot(expert_rows.T, gate_pre_grad, preferred_element_type=jnp.float32)
    up_grad = jnp.dot(expert_rows.T, up_pre_grad, preferred_element_type=jnp.float32)
    return input_grad, product, gate_grad, up_grad, down_grad


def reference(tokens, cotangent, routing, gate_weights, gate_proj, up_proj, down_proj):
    pair_count = TOKENS * TOP
    row_limit = N_EP * CAP
    pair_expert = routing.reshape(pair_count)
    pair_weight = gate_weights.reshape(pair_count)

    def one_expert(expert_index):
        chosen = jnp.nonzero(pair_expert == expert_index, size=row_limit, fill_value=pair_count)[0].astype(jnp.int32)
        is_valid = chosen < pair_count
        safe_index = jnp.where(is_valid, chosen, 0).astype(jnp.int32)
        token_index = (safe_index // TOP).astype(jnp.int32)
        expert_rows = jnp.where(is_valid[:, None], tokens[token_index], jnp.zeros((), tokens.dtype))
        weight = jnp.where(is_valid, pair_weight[safe_index], jnp.zeros((), pair_weight.dtype))
        scaled = (weight[:, None] * cotangent[token_index].astype(jnp.float32)).astype(jnp.bfloat16)
        terms = expert_pass(expert_rows, scaled, gate_proj[expert_index], up_proj[expert_index], down_proj[expert_index])
        return (chosen,) + terms

    chosen, input_grad, product, gate_grad, up_grad, down_grad = lax.map(one_expert, jnp.arange(EXPERTS, dtype=jnp.int32))
    flat_chosen = chosen.reshape(-1)
    pair_grad = jnp.zeros((pair_count + 1, D), jnp.float32).at[flat_chosen].set(input_grad.reshape(-1, D))
    pair_product = jnp.zeros((pair_count + 1,), jnp.float32).at[flat_chosen].set(product.reshape(-1))
    tokens_grad = jnp.sum(pair_grad[:pair_count].reshape(TOKENS, TOP, D), axis=1).astype(jnp.bfloat16)
    gates_grad = (pair_product[:pair_count] / pair_weight).reshape(TOKENS, TOP)
    return tokens_grad, gates_grad, gate_grad, up_grad, down_grad
```

```python
import jax
import jax.numpy as jnp
from jax import lax
from jax.experimental import pallas as pl
from jax.experimental.pallas import tpu as pltpu
from jax.sharding import PartitionSpec as P

F32 = jnp.float32
BF16 = jnp.bfloat16
LANES = 128
VMEM = pltpu.VMEM
SMEM = pltpu.SMEM


def mm(a, b, dims):
    return lax.dot_general(a, b, (dims, ((), ())), preferred_element_type=F32)


def dispatch_kernel(
    experts, local_experts, quarter, member, routing, weights, tokens, cotangent, rows_out, pick
):
    token_count = tokens.shape[0]
    row_count = rows_out.shape[0]
    slots = row_count // 2
    lane = lax.broadcasted_iota(jnp.int32, (token_count, experts), 1)
    chosen = [routing[:, k : k + 1] for k in range(2)]
    onehot = [jnp.where(lane == c, 1.0, 0.0) for c in chosen]
    earlier = lax.broadcasted_iota(jnp.int32, (token_count, token_count), 0)
    later = lax.broadcasted_iota(jnp.int32, (token_count, token_count), 1)
    lower = jnp.where(earlier > later, 1.0, 0.0).astype(BF16)
    before = mm(lower, (onehot[0] + onehot[1]).astype(BF16), ((1,), (0,)))
    row = lax.broadcasted_iota(jnp.int32, (token_count, row_count), 1)
    slot = lax.broadcasted_iota(jnp.int32, (token_count, slots), 1)
    cot = cotangent[...].astype(F32)
    total = None
    token_pick = None
    per_device = local_experts * quarter
    for k in range(2):
        position = jnp.sum(onehot[k] * before, axis=1, keepdims=True).astype(jnp.int32)
        local = position - member[0] * quarter
        present = (local >= 0) & (local < quarter)
        device = chosen[k] // local_experts
        within = (chosen[k] - device * local_experts) * quarter + local
        slot_of = jnp.where(present, device * per_device + within, -1)
        pick[k] = jnp.where(slot == slot_of, 1.0, 0.0).astype(BF16)
        token_row = jnp.where(present, device * (2 * per_device) + within, -1)
        scaled_row = jnp.where(present, device * (2 * per_device) + per_device + within, -1)
        hit = jnp.where(row == token_row, 1.0, 0.0)
        token_pick = hit if token_pick is None else token_pick + hit
        scaled = (weights[:, k : k + 1] * cot).astype(BF16)
        part = mm(jnp.where(row == scaled_row, 1.0, 0.0).astype(BF16), scaled, ((0,), (0,)))
        total = part if total is None else total + part
    total = total + mm(token_pick.astype(BF16), tokens[...], ((0,), (0,)))
    rows_out[...] = total.astype(BF16)


def hidden_terms(rows, scaled, gate, up, down):
    gate_pre = mm(rows, gate, ((1,), (0,))).astype(BF16).astype(F32)
    up_pre = mm(rows, up, ((1,), (0,))).astype(BF16).astype(F32)
    hidden_grad = mm(scaled, down, ((1,), (1,)))
    sigmoid = jax.nn.sigmoid(gate_pre)
    activated = gate_pre * sigmoid
    hidden = activated * up_pre
    gate_grad = (hidden_grad * up_pre * sigmoid * (1.0 + gate_pre * (1.0 - sigmoid))).astype(BF16)
    up_grad = (hidden_grad * activated).astype(BF16)
    return hidden, hidden_grad, gate_grad, up_grad


def input_kernel(rows, scaled, gate, up, down, out):
    width = rows.shape[-1]
    hidden, hidden_grad, gate_grad, up_grad = hidden_terms(
        rows[0, 0], scaled[0, 0], gate[0, 0], up[0, 0], down[0, 0]
    )
    product = jnp.sum(hidden_grad * hidden, axis=1, keepdims=True)
    grad = mm(gate_grad, gate[0, 0], ((1,), (1,))) + mm(up_grad, up[0, 0], ((1,), (1,)))
    tail = jnp.broadcast_to(product, (product.shape[0], LANES))

    @pl.when(pl.program_id(1) == 0)
    def _():
        out[0, :, :width] = grad
        out[0, :, width:] = tail

    @pl.when(pl.program_id(1) != 0)
    def _():
        out[0, :, :width] += grad
        out[0, :, width:] += tail


def weight_kernel(rows, scaled, gate, up, down, gate_out, up_out, down_out):
    own_rows, own_scaled = rows[0, 0, 0], scaled[0, 0, 0]
    hidden, _, gate_grad, up_grad = hidden_terms(own_rows, own_scaled, gate[0], up[0], down[0])
    gate_part = mm(own_rows, gate_grad, ((0,), (0,)))
    up_part = mm(own_rows, up_grad, ((0,), (0,)))
    down_part = mm(hidden.astype(BF16), own_scaled, ((0,), (0,)))

    @pl.when(pl.program_id(1) == 0)
    def _():
        gate_out[0] = gate_part
        up_out[0] = up_part
        down_out[0] = down_part

    @pl.when(pl.program_id(1) != 0)
    def _():
        gate_out[0] += gate_part
        up_out[0] += up_part
        down_out[0] += down_part


def split3(value):
    high = value.astype(BF16)
    rest = value - high.astype(F32)
    middle = rest.astype(BF16)
    low = (rest - middle.astype(F32)).astype(BF16)
    return high, middle, low


def combine_kernel(back, pick, grad_out, product_out):
    width = grad_out.shape[-1]
    both = pick[0] + pick[1]
    dims = ((1,), (0,))
    grad_out[...] = sum(mm(both, part, dims) for part in split3(back[:, :width]))
    tails = split3(back[:, width:])
    first = sum(mm(pick[0], part, dims) for part in tails)
    second = sum(mm(pick[1], part, dims) for part in tails)
    lane = lax.broadcasted_iota(jnp.int32, first.shape, 1)
    product_out[...] = jnp.where(lane == 0, first, second)


def shards(tokens, cotangent, routing, gate_weights, gate_proj, up_proj, down_proj):
    token_count, model_width = tokens.shape
    top_count = routing.shape[1]
    local_experts, _, hidden_width = gate_proj.shape
    groups = lax.axis_size("ep")
    members = lax.axis_size("tp")
    experts = local_experts * groups
    capacity = members * (
        (3 * token_count * top_count + experts * members - 1) // (experts * members)
    )
    quarter = capacity // members
    slots = experts * quarter
    own = groups * quarter
    member = lax.axis_index("tp").astype(jnp.int32).reshape(1)

    gate_all = lax.all_gather(gate_proj, "tp")
    up_all = lax.all_gather(up_proj, "tp")
    down_all = lax.all_gather(down_proj, "tp")

    whole = pl.BlockSpec(memory_space=VMEM)
    send, pick = pl.pallas_call(
        lambda *refs: dispatch_kernel(experts, local_experts, quarter, *refs),
        out_shape=(
            jax.ShapeDtypeStruct((2 * slots, model_width), BF16),
            jax.ShapeDtypeStruct((2, token_count, slots), BF16),
        ),
        in_specs=[pl.BlockSpec(memory_space=SMEM), whole, whole, whole, whole],
        out_specs=(whole, whole),
        name="dispatch",
    )(member, routing, gate_weights, tokens, cotangent)
    send = send.reshape(groups, 2, local_experts, quarter, model_width)
    landed = lax.all_to_all(send, "ep", split_axis=0, concat_axis=0, tiled=True)
    own_rows = landed.transpose(1, 2, 0, 3, 4).reshape(2, local_experts, own, model_width)
    all_rows = lax.all_gather(own_rows, "tp")

    tail_width = model_width + LANES
    grid = (local_experts, members)
    back = pl.pallas_call(
        input_kernel,
        grid=grid,
        out_shape=jax.ShapeDtypeStruct((local_experts, own, tail_width), F32),
        in_specs=[
            pl.BlockSpec((1, 1, own, model_width), lambda e, t: (0, e, 0, 0)),
            pl.BlockSpec((1, 1, own, model_width), lambda e, t: (1, e, 0, 0)),
            pl.BlockSpec((1, 1, model_width, hidden_width), lambda e, t: (t, e, 0, 0)),
            pl.BlockSpec((1, 1, model_width, hidden_width), lambda e, t: (t, e, 0, 0)),
            pl.BlockSpec((1, 1, hidden_width, model_width), lambda e, t: (t, e, 0, 0)),
        ],
        out_specs=pl.BlockSpec((1, own, tail_width), lambda e, t: (e, 0, 0)),
        name="input_grad",
    )(own_rows, own_rows, gate_all, up_all, down_all)
    back = back.reshape(local_experts, groups, quarter, tail_width).transpose(1, 0, 2, 3)
    back = lax.all_to_all(back, "ep", split_axis=0, concat_axis=0, tiled=True)
    token_grad, product = pl.pallas_call(
        combine_kernel,
        out_shape=(
            jax.ShapeDtypeStruct((token_count, model_width), F32),
            jax.ShapeDtypeStruct((token_count, LANES), F32),
        ),
        in_specs=[whole, whole],
        out_specs=(whole, whole),
        name="combine",
    )(back.reshape(slots, tail_width), pick)
    total_grad, total_product = lax.psum((token_grad, product[:, :top_count]), "tp")
    tokens_grad = total_grad.astype(BF16)
    gates_grad = total_product / gate_weights

    gate_grad, up_grad, down_grad = pl.pallas_call(
        weight_kernel,
        grid=grid,
        out_shape=(
            jax.ShapeDtypeStruct((local_experts, model_width, hidden_width), F32),
            jax.ShapeDtypeStruct((local_experts, model_width, hidden_width), F32),
            jax.ShapeDtypeStruct((local_experts, hidden_width, model_width), F32),
        ),
        in_specs=[
            pl.BlockSpec((1, 1, 1, own, model_width), lambda e, t: (t, 0, e, 0, 0)),
            pl.BlockSpec((1, 1, 1, own, model_width), lambda e, t: (t, 1, e, 0, 0)),
            pl.BlockSpec((1, model_width, hidden_width), lambda e, t: (e, 0, 0)),
            pl.BlockSpec((1, model_width, hidden_width), lambda e, t: (e, 0, 0)),
            pl.BlockSpec((1, hidden_width, model_width), lambda e, t: (e, 0, 0)),
        ],
        out_specs=(
            pl.BlockSpec((1, model_width, hidden_width), lambda e, t: (e, 0, 0)),
            pl.BlockSpec((1, model_width, hidden_width), lambda e, t: (e, 0, 0)),
            pl.BlockSpec((1, hidden_width, model_width), lambda e, t: (e, 0, 0)),
        ),
        name="weight_grad",
    )(all_rows, all_rows, gate_proj, up_proj, down_proj)
    return (tokens_grad, gates_grad, gate_grad, up_grad, down_grad)


def solution(mesh):
    in_specs = (
        P("ep", None),
        P("ep", None),
        P("ep", None),
        P("ep", None),
        P("ep", None, "tp"),
        P("ep", None, "tp"),
        P("ep", "tp", None),
    )
    out_specs = (
        P("ep", None),
        P("ep", None),
        P("ep", None, "tp"),
        P("ep", None, "tp"),
        P("ep", "tp", None),
    )
    return jax.shard_map(shards, mesh=mesh, in_specs=in_specs, out_specs=out_specs, check_vma=False)
```

```python
import jax
import jax.numpy as jnp
from jax import lax
from jax.experimental import pallas as pl
from jax.experimental.pallas import tpu as pltpu
from jax.sharding import PartitionSpec as P

F32 = jnp.float32
F16 = jnp.float16
BF16 = jnp.bfloat16
I32 = jnp.int32
LANES = 128
HALVES = 2
SPREAD = 16384.0
VMEM = pltpu.VMEM
SMEM = pltpu.SMEM
NN = ((1,), (0,))
NT = ((1,), (1,))
TN = ((0,), (0,))


def mm(a, b, dims=NN):
    return lax.dot_general(a, b, (dims, ((), ())), preferred_element_type=F32)


def iota(shape, dim):
    return lax.broadcasted_iota(I32, shape, dim)


def split3(value):
    high = value.astype(BF16)
    rest = value - high.astype(F32)
    middle = rest.astype(BF16)
    low = (rest - middle.astype(F32)).astype(BF16)
    return high, middle, low


def exponent(value):
    return jnp.floor(jnp.log(jnp.maximum(value, 1e-30)) * 1.4426950408889634)


def dispatch_kernel(
    experts, local_experts, quarter, member, routing, weights, tokens, cotangent, rows_out, pick
):
    token_count, width = tokens.shape
    half = width // HALVES
    row_count = rows_out.shape[0]
    slots = pick.shape[1]
    group = local_experts * quarter
    chunk = HALVES * 2 * group
    expert = iota((experts, token_count), 0)
    chosen = [routing[k : k + 1, :] for k in range(2)]
    onehot = [jnp.where(expert == c, 1.0, 0.0) for c in chosen]
    earlier = iota((token_count, token_count), 0)
    later = iota((token_count, token_count), 1)
    upper = jnp.where(earlier < later, 1.0, 0.0).astype(BF16)
    before = mm((onehot[0] + onehot[1]).astype(BF16), upper)
    row = iota((row_count, token_count), 0)
    slot = iota((slots, token_count), 0)
    token_rows = []
    for k in range(2):
        position = jnp.sum(onehot[k] * before, axis=0, keepdims=True).astype(I32)
        local = position - member[0] * quarter
        present = (local >= 0) & (local < quarter)
        device = chosen[k] // local_experts
        within = (chosen[k] - device * local_experts) * quarter + local
        pick[k] = jnp.where(slot == jnp.where(present, device * group + within, -1), 1.0, 0.0).astype(BF16)
        token_rows.append(jnp.where(present, device * chunk + within, -chunk))
    total = None
    for h in range(HALVES):
        columns = slice(h * half, (h + 1) * half)
        base = h * 2 * group
        hits = [jnp.where(row == r + base, 1.0, 0.0) for r in token_rows]
        part = mm((hits[0] + hits[1]).astype(BF16), tokens[:, columns])
        hits = [jnp.where(row == r + (base + group), 1.0, 0.0) for r in token_rows]
        slot_weight = jnp.sum(hits[0] * weights[0:1, :] + hits[1] * weights[1:2, :], axis=1, keepdims=True)
        part = part + slot_weight * mm((hits[0] + hits[1]).astype(BF16), cotangent[:, columns])
        total = part if total is None else total + part
    rows_out[...] = total.astype(BF16)


def land(source, expert, local_experts, quarter, rows, scaled, offset):
    half = source.shape[1]
    group = local_experts * quarter
    chunk = HALVES * 2 * group
    devices = 16
    out_rows = devices * quarter
    index = iota((HALVES * 2 * out_rows, devices * chunk), 0)
    column = iota((HALVES * 2 * out_rows, devices * chunk), 1)
    kind = index // out_rows
    rest = index - kind * out_rows
    device = rest // quarter
    wanted = device * chunk + kind * group + expert * quarter + (rest - device * quarter)
    permutation = jnp.where(column == wanted, 1.0, 0.0).astype(BF16)
    for block in range(source.shape[0] // (devices * chunk)):
        moved = mm(permutation, source[block * devices * chunk : (block + 1) * devices * chunk, :])
        moved = moved.astype(BF16)
        at = slice(offset + block * out_rows, offset + (block + 1) * out_rows)
        for h in range(HALVES):
            columns = slice(h * half, (h + 1) * half)
            first = 2 * h * out_rows
            rows[at, columns] = moved[first : first + out_rows]
            scaled[at, columns] = moved[first + out_rows : first + 2 * out_rows]


def hidden_terms(gate_pre, up_pre, hidden_grad):
    gate_pre = gate_pre.astype(BF16).astype(F32)
    up_pre = up_pre.astype(BF16).astype(F32)
    sigmoid = jax.nn.sigmoid(gate_pre)
    activated = gate_pre * sigmoid
    hidden = activated * up_pre
    gate_grad = (hidden_grad * up_pre * sigmoid * (1.0 + gate_pre * (1.0 - sigmoid))).astype(BF16)
    up_grad = (hidden_grad * activated).astype(BF16)
    return hidden, gate_grad, up_grad


def input_kernel(local_experts, quarter, landed, *refs):
    gates, ups, downs = refs[0:4], refs[4:8], refs[8:11]
    down_even, down_odd, out, rows, scaled = refs[11:]
    width = rows.shape[1]
    expert = pl.program_id(0)
    land(landed, expert, local_experts, quarter, rows, scaled, 0)
    gate = jnp.concatenate([g[0] for g in gates], axis=1)
    up = jnp.concatenate([u[0] for u in ups], axis=1)
    last = jnp.where(expert == 0, down_even[0], down_odd[0])
    down = jnp.concatenate([d[0] for d in downs] + [last], axis=0)
    hidden_grad = mm(scaled[...], down, NT)
    hidden, gate_grad, up_grad = hidden_terms(mm(rows[...], gate), mm(rows[...], up), hidden_grad)
    product = jnp.sum(hidden_grad * hidden, axis=1, keepdims=True)
    grad = mm(gate_grad, gate, NT) + mm(up_grad, up, NT)
    power = exponent(jnp.max(jnp.abs(grad), axis=1, keepdims=True))
    out[0, :, :width] = grad * (SPREAD * jnp.exp2(-power))
    product_power = exponent(jnp.abs(product))
    product = product * jnp.exp2(-product_power)
    high = product.astype(BF16).astype(F32)
    low = (product - high) * 256.0
    lane = iota((product.shape[0], LANES), 1)
    out[0, :, width:] = jnp.where(
        lane == 0,
        power,
        jnp.where(lane == 1, product_power, jnp.where(lane == 2, high, low)),
    )


def weight_kernel(local_experts, quarter, *refs):
    sources, (gate, up, down), (gate_out, up_out, down_out) = refs[0:5], refs[5:8], refs[8:11]
    rows, scaled = refs[11:]
    expert = pl.program_id(0)
    offset = 0
    chunk = HALVES * 2 * local_experts * quarter
    for source in sources:
        land(source, expert, local_experts, quarter, rows, scaled, offset)
        offset += source.shape[0] // chunk * quarter
    hidden_width = gate.shape[2]
    both = mm(rows[...], jnp.concatenate([gate[0], up[0]], axis=1))
    hidden_grad = mm(scaled[...], down[0], NT)
    hidden, gate_grad, up_grad = hidden_terms(both[:, :hidden_width], both[:, hidden_width:], hidden_grad)
    grads = mm(rows[...], jnp.concatenate([gate_grad, up_grad], axis=1), TN)
    gate_out[0] = grads[:, :hidden_width]
    up_out[0] = grads[:, hidden_width:]
    down_out[0] = mm(hidden.astype(BF16), scaled[...], TN)


def combine_kernel(back, pick, grad_out, product_out):
    width = grad_out.shape[-1]
    both = pick[0] + pick[1]
    power = back[:, width : width + 1]
    grad = back[:, :width] * (jnp.exp2(power) * (1.0 / SPREAD))
    grad_out[...] = sum(mm(both, part, TN) for part in split3(grad))
    high, low = back[:, width + 2 : width + 3], back[:, width + 3 : width + 4]
    product = (high + low * (1.0 / 256.0)) * jnp.exp2(back[:, width + 1 : width + 2])
    parts = split3(jnp.broadcast_to(product, (product.shape[0], LANES)))
    first = sum(mm(pick[0], part, TN) for part in parts)
    second = sum(mm(pick[1], part, TN) for part in parts)
    lane = iota(first.shape, 1)
    product_out[...] = jnp.where(lane == 0, first, second)


def shards(tokens, cotangent, routing, gate_weights, gate_proj, up_proj, down_proj):
    token_count, model_width = tokens.shape
    top_count = routing.shape[1]
    local_experts, _, hidden_width = gate_proj.shape
    groups = lax.axis_size("ep")
    members = lax.axis_size("tp")
    experts = local_experts * groups
    capacity = members * (
        (3 * token_count * top_count + experts * members - 1) // (experts * members)
    )
    quarter = capacity // members
    slots = experts * quarter
    own = groups * quarter
    chunk = HALVES * 2 * local_experts * quarter
    half = model_width // HALVES
    member = lax.axis_index("tp").astype(I32).reshape(1)
    right = [(i, (i + 1) % members) for i in range(members)]
    left = [(i, (i - 1) % members) for i in range(members)]

    gates, ups, downs = [gate_proj], [up_proj], [down_proj]
    for kept, mine in ((gates, gate_proj), (ups, up_proj), (downs, down_proj)):
        kept.append(lax.ppermute(mine, "tp", right))
        kept.append(lax.ppermute(mine, "tp", left))
    gates.append(lax.ppermute(gates[2], "tp", left))
    ups.append(lax.ppermute(ups[1], "tp", right))
    down_even = lax.ppermute(downs[2][0:1], "tp", left)
    down_odd = lax.ppermute(downs[1][1:2], "tp", right)

    whole = pl.BlockSpec(memory_space=VMEM)
    send, pick = pl.pallas_call(
        lambda *refs: dispatch_kernel(experts, local_experts, quarter, *refs),
        out_shape=(
            jax.ShapeDtypeStruct((groups * chunk, half), BF16),
            jax.ShapeDtypeStruct((2, slots, token_count), BF16),
        ),
        in_specs=[pl.BlockSpec(memory_space=SMEM), whole, whole, whole, whole],
        out_specs=(whole, whole),
        name="dispatch",
    )(member, routing.T, gate_weights.T, tokens, cotangent)
    landed = lax.all_to_all(
        send.reshape(groups, chunk, half), "ep", split_axis=0, concat_axis=0, tiled=True
    ).reshape(groups * chunk, half)

    from_left = lax.ppermute(landed, "tp", right)
    from_right = lax.ppermute(landed, "tp", left)
    middle = groups * chunk // 2
    opposite_low = lax.ppermute(from_right[:middle], "tp", left)
    opposite_high = lax.ppermute(from_left[middle:], "tp", right)

    tail_width = model_width + LANES
    spec_in = pl.BlockSpec((1, model_width, hidden_width), lambda e: (e, 0, 0))
    spec_down = pl.BlockSpec((1, hidden_width, model_width), lambda e: (e, 0, 0))
    spec_one = pl.BlockSpec((1, hidden_width, model_width), lambda e: (0, 0, 0))

    def rows_spec(array):
        return pl.BlockSpec(array.shape, lambda e: (0, 0))

    back = pl.pallas_call(
        lambda *refs: input_kernel(local_experts, quarter, *refs),
        grid=(local_experts,),
        out_shape=jax.ShapeDtypeStruct((local_experts, own, tail_width), F32),
        in_specs=[rows_spec(landed)] + [spec_in] * 8 + [spec_down] * 3 + [spec_one] * 2,
        out_specs=pl.BlockSpec((1, own, tail_width), lambda e: (e, 0, 0)),
        scratch_shapes=[VMEM((own, model_width), BF16)] * 2,
        name="input_grad",
    )(landed, *gates, *ups, *downs, down_even, down_odd)
    back = back.astype(F16).reshape(local_experts, groups, quarter, tail_width).transpose(1, 0, 2, 3)
    back = lax.all_to_all(back, "ep", split_axis=0, concat_axis=0, tiled=True)
    back = back.astype(F32).reshape(slots, tail_width)
    token_grad, product = pl.pallas_call(
        combine_kernel,
        out_shape=(
            jax.ShapeDtypeStruct((token_count, model_width), F32),
            jax.ShapeDtypeStruct((token_count, LANES), F32),
        ),
        in_specs=[whole, whole],
        out_specs=(whole, whole),
        name="combine",
    )(back, pick)
    total_grad, total_product = lax.psum((token_grad, product[:, :top_count]), "tp")
    tokens_grad = total_grad.astype(BF16)
    gates_grad = total_product / gate_weights

    sources = (landed, from_left, from_right, opposite_low, opposite_high)
    all_rows = members * own
    gate_grad, up_grad, down_grad = pl.pallas_call(
        lambda *refs: weight_kernel(local_experts, quarter, *refs),
        grid=(local_experts,),
        out_shape=(
            jax.ShapeDtypeStruct((local_experts, model_width, hidden_width), F32),
            jax.ShapeDtypeStruct((local_experts, model_width, hidden_width), F32),
            jax.ShapeDtypeStruct((local_experts, hidden_width, model_width), F32),
        ),
        in_specs=[rows_spec(s) for s in sources] + [spec_in, spec_in, spec_down],
        out_specs=(spec_in, spec_in, spec_down),
        scratch_shapes=[VMEM((all_rows, model_width), BF16)] * 2,
        name="weight_grad",
    )(*sources, gate_proj, up_proj, down_proj)
    return (tokens_grad, gates_grad, gate_grad, up_grad, down_grad)


def solution(mesh):
    in_specs = (
        P("ep", None),
        P("ep", None),
        P("ep", None),
        P("ep", None),
        P("ep", None, "tp"),
        P("ep", None, "tp"),
        P("ep", "tp", None),
    )
    out_specs = (
        P("ep", None),
        P("ep", None),
        P("ep", None, "tp"),
        P("ep", None, "tp"),
        P("ep", "tp", None),
    )
    return jax.shard_map(shards, mesh=mesh, in_specs=in_specs, out_specs=out_specs, check_vma=False)
```

```python
import jax
import jax.numpy as jnp
from jax import lax
from jax.experimental import pallas as pl
from jax.experimental.pallas import tpu as pltpu
from jax.sharding import PartitionSpec as P


F32 = jnp.float32
F16 = jnp.float16
BF16 = jnp.bfloat16
I32 = jnp.int32
LANES = 128
SUBLANES = 8
BLOCK = 16
HALVES = 2
SPREAD = 16384.0
VMEM = pltpu.VMEM
SMEM = pltpu.SMEM
NN = ((1,), (0,))
NT = ((1,), (1,))
TN = ((0,), (0,))


def mm(a, b, dims=NN):
    return lax.dot_general(a, b, (dims, ((), ())), preferred_element_type=F32)


def iota(shape, dim):
    return lax.broadcasted_iota(I32, shape, dim)


def split3(value):
    high = value.astype(BF16)
    rest = value - high.astype(F32)
    middle = rest.astype(BF16)
    low = (rest - middle.astype(F32)).astype(BF16)
    return high, middle, low


def exponent(value):
    return jnp.floor(jnp.log(jnp.maximum(value, 1e-30)) * 1.4426950408889634)


def dispatch_kernel(
    experts, local_experts, quarter, member, routing, weights, tokens, cotangent, rows_out, pick
):
    token_count, width = tokens.shape
    half = width // HALVES
    row_count = rows_out.shape[0]
    slots = pick.shape[1]
    group = local_experts * quarter
    chunk = HALVES * 2 * group
    devices = experts // local_experts
    expert = iota((experts, token_count), 0)
    chosen = [routing[k : k + 1, :] for k in range(2)]
    onehot = [jnp.where(expert == c, 1.0, 0.0) for c in chosen]
    earlier = iota((token_count, token_count), 0)
    later = iota((token_count, token_count), 1)
    upper = jnp.where(earlier < later, 1.0, 0.0).astype(BF16)
    before = mm((onehot[0] + onehot[1]).astype(BF16), upper)
    row = iota((row_count, token_count), 0)
    slot = iota((slots, token_count), 0)
    token_rows = []
    for k in range(2):
        position = jnp.sum(onehot[k] * before, axis=0, keepdims=True).astype(I32)
        local = position - member[0] * quarter
        present = (local >= 0) & (local < quarter)
        device = chosen[k] // local_experts
        within = (chosen[k] - device * local_experts) * quarter + local
        pick[k] = jnp.where(slot == jnp.where(present, within * devices + device, -1), 1.0, 0.0).astype(BF16)
        token_rows.append(jnp.where(present, device * chunk + within, -chunk))
    total = None
    for h in range(HALVES):
        columns = slice(h * half, (h + 1) * half)
        base = h * 2 * group
        hits = [jnp.where(row == r + base, 1.0, 0.0) for r in token_rows]
        part = mm((hits[0] + hits[1]).astype(BF16), tokens[:, columns])
        hits = [jnp.where(row == r + (base + group), 1.0, 0.0) for r in token_rows]
        slot_weight = jnp.sum(hits[0] * weights[0:1, :] + hits[1] * weights[1:2, :], axis=1, keepdims=True)
        part = part + slot_weight * mm((hits[0] + hits[1]).astype(BF16), cotangent[:, columns])
        total = part if total is None else total + part
    rows_out[...] = total.astype(BF16)


def land(source, expert, local_experts, quarter, rows, scaled, offset):
    half = source.shape[1]
    group = local_experts * quarter
    chunk = HALVES * 2 * group
    out_rows = BLOCK * quarter
    index = iota((HALVES * 2 * out_rows, 1), 0)
    kind = index // out_rows
    rest = index - kind * out_rows
    slot = rest // BLOCK
    wanted = (rest - slot * BLOCK) * chunk + kind * group + expert * quarter + slot
    column = iota((HALVES * 2 * out_rows, BLOCK * chunk), 1)
    permutation = jnp.where(column == wanted, 1.0, 0.0).astype(BF16)
    for block in range(source.shape[0] // (BLOCK * chunk)):
        moved = mm(permutation, source[block * BLOCK * chunk : (block + 1) * BLOCK * chunk, :])
        moved = moved.astype(BF16)
        at = slice(offset + block * out_rows, offset + (block + 1) * out_rows)
        for h in range(HALVES):
            columns = slice(h * half, (h + 1) * half)
            first = 2 * h * out_rows
            rows[at, columns] = moved[first : first + out_rows]
            scaled[at, columns] = moved[first + out_rows : first + 2 * out_rows]


def hidden_terms(gate_pre, up_pre, hidden_grad):
    gate_pre = gate_pre.astype(BF16).astype(F32)
    up_pre = up_pre.astype(BF16).astype(F32)
    sigmoid = jax.nn.sigmoid(gate_pre)
    activated = gate_pre * sigmoid
    hidden = activated * up_pre
    gate_grad = (hidden_grad * up_pre * sigmoid * (1.0 + gate_pre * (1.0 - sigmoid))).astype(BF16)
    up_grad = (hidden_grad * activated).astype(BF16)
    return hidden, gate_grad, up_grad


def input_kernel(local_experts, quarter, landed, *refs):
    gates, ups, downs = refs[0:4], refs[4:8], refs[8:11]
    down_even, down_odd, out, rows, scaled = refs[11:]
    own, _ = rows.shape
    slots = local_experts * quarter
    devices = own // quarter
    stride = (slots + 1) * SUBLANES
    for i in range(slots, SUBLANES):
        at = slots * SUBLANES + i
        out[pl.ds(at, devices, stride=stride), :] = jnp.zeros((devices, LANES), F32)
    for expert in range(local_experts):
        land(landed, expert, local_experts, quarter, rows, scaled, 0)
        gate = jnp.concatenate([g[expert] for g in gates], axis=1)
        up = jnp.concatenate([u[expert] for u in ups], axis=1)
        last = (down_even, down_odd)[expert][0]
        down = jnp.concatenate([d[expert] for d in downs] + [last], axis=0)
        hidden_grad = mm(scaled[...], down, NT)
        hidden, gate_grad, up_grad = hidden_terms(mm(rows[...], gate), mm(rows[...], up), hidden_grad)
        product = jnp.sum(hidden_grad * hidden, axis=1, keepdims=True)
        grad = mm(gate_grad, gate, NT) + mm(up_grad, up, NT)
        power = exponent(jnp.max(jnp.abs(grad), axis=1, keepdims=True))
        grad = grad * (SPREAD * jnp.exp2(-power))
        product_power = exponent(jnp.abs(product))
        product = product * jnp.exp2(-product_power)
        high = product.astype(BF16).astype(F32)
        low = (product - high) * 256.0
        lane = iota((own, LANES), 1)
        tail = jnp.where(
            lane == 0,
            power,
            jnp.where(lane == 1, product_power, jnp.where(lane == 2, high, low)),
        )
        for block in range(devices // BLOCK):
            for q in range(quarter):
                at = (block * quarter + q) * BLOCK
                to = block * BLOCK * stride
                slot = expert * quarter + q
                for i in range(SUBLANES):
                    piece = grad[at : at + BLOCK, i * LANES : (i + 1) * LANES]
                    out[pl.ds(to + slot * SUBLANES + i, BLOCK, stride=stride), :] = piece
                to += slots * SUBLANES + slot
                out[pl.ds(to, BLOCK, stride=stride), :] = tail[at : at + BLOCK]


def weight_kernel(local_experts, quarter, *refs):
    sources, (gate, up, down), (gate_out, up_out, down_out) = refs[0:5], refs[5:8], refs[8:11]
    rows, scaled = refs[11:]
    chunk = HALVES * 2 * local_experts * quarter
    hidden_width = gate.shape[2]
    for expert in range(local_experts):
        offset = 0
        for source in sources:
            land(source, expert, local_experts, quarter, rows, scaled, offset)
            offset += source.shape[0] // chunk * quarter
        both = mm(rows[...], jnp.concatenate([gate[expert], up[expert]], axis=1))
        hidden_grad = mm(scaled[...], down[expert], NT)
        hidden, gate_grad, up_grad = hidden_terms(
            both[:, :hidden_width], both[:, hidden_width:], hidden_grad
        )
        grads = mm(rows[...], jnp.concatenate([gate_grad, up_grad], axis=1), TN)
        gate_out[expert] = grads[:, :hidden_width]
        up_out[expert] = grads[:, hidden_width:]
        down_out[expert] = mm(hidden.astype(BF16), scaled[...], TN)


def member_rows(member, distance, members, count):
    return pl.ds(pl.multiple_of(lax.rem(member + distance, members) * count, count), count)


def combine_kernel(members, devices, member, back, pick, *refs):
    outs, total = refs[:-1], refs[-1]
    token_count, width = total.shape
    slots = pick.shape[1] // devices
    stride = (slots + 1) * SUBLANES
    tails = [
        back[pl.ds(slots * SUBLANES + slot, devices, stride=stride), :] for slot in range(slots)
    ]
    tail = jnp.concatenate(tails, axis=0)
    scale = jnp.exp2(tail[:, 0:1]) * (1.0 / SPREAD)
    columns = []
    for i in range(SUBLANES):
        pieces = [
            back[pl.ds(slot * SUBLANES + i, devices, stride=stride), :] for slot in range(slots)
        ]
        columns.append(jnp.concatenate(pieces, axis=0))
    grad = jnp.concatenate(columns, axis=1) * scale
    both = pick[0] + pick[1]
    total[...] = sum(mm(both, part, TN) for part in split3(grad))
    product = (tail[:, 2:3] + tail[:, 3:4] * (1.0 / 256.0)) * jnp.exp2(tail[:, 1:2])
    sums = [jnp.sum(pick[k].astype(F32) * product, axis=0, keepdims=True) for k in range(2)]
    spare = jnp.zeros((1, width - 2 * token_count), F32)
    line = jnp.broadcast_to(jnp.concatenate(sums + [spare], axis=1), (SUBLANES, width))
    count = token_count // members
    for out, distance in zip(outs, (0, 1, 3, 2)):
        out[0:count, :] = total[member_rows(member[0], distance, members, count), :]
        out[count : count + SUBLANES, :] = line


def sum_kernel(own, from_left, from_right, from_opposite, weights, grad_out, gates_out):
    count = grad_out.shape[0]
    token_count = weights.shape[1]
    total = (own[...] + from_opposite[...]) + (from_left[...] + from_right[...])
    grad_out[...] = total[0:count].astype(BF16)
    for k in range(2):
        product = total[count : count + 1, k * token_count : (k + 1) * token_count]
        gates_out[k : k + 1, :] = product / weights[k : k + 1, :]


def place_kernel(members, member, own, from_left, from_right, from_opposite, out):
    count = own.shape[0]
    for piece, distance in ((own, 0), (from_left, 3), (from_right, 1), (from_opposite, 2)):
        out[member_rows(member[0], distance, members, count), :] = piece[...]


def step(tokens, cotangent, routing, gate_weights, gate_proj, up_proj, down_proj):
    token_count, model_width = tokens.shape
    top_count = routing.shape[1]
    local_experts, _, hidden_width = gate_proj.shape
    groups = lax.axis_size("ep")
    members = lax.axis_size("tp")
    experts = local_experts * groups
    capacity = members * (
        (3 * token_count * top_count + experts * members - 1) // (experts * members)
    )
    quarter = capacity // members
    slots = experts * quarter
    own = groups * quarter
    chunk = HALVES * 2 * local_experts * quarter
    half = model_width // HALVES
    member = lax.axis_index("tp").astype(I32).reshape(1)
    right = [(i, (i + 1) % members) for i in range(members)]
    left = [(i, (i - 1) % members) for i in range(members)]
    across = [(i, (i + 2) % members) for i in range(members)]
    whole = pl.BlockSpec(memory_space=VMEM)
    scalar = pl.BlockSpec(memory_space=SMEM)

    def call(kernel, out_shape, args, scalars=0, scratch=()):
        return pl.pallas_call(
            kernel,
            out_shape=out_shape,
            in_specs=[scalar] * scalars + [whole] * (len(args) - scalars),
            out_specs=jax.tree.map(lambda _: whole, out_shape),
            scratch_shapes=list(scratch),
        )(*args)

    def shape(dims, dtype):
        return jax.ShapeDtypeStruct(dims, dtype)

    gates, ups, downs = [gate_proj], [up_proj], [down_proj]
    for kept, mine in ((gates, gate_proj), (ups, up_proj), (downs, down_proj)):
        kept.append(lax.ppermute(mine, "tp", right))
        kept.append(lax.ppermute(mine, "tp", left))
    gates.append(lax.ppermute(gates[2], "tp", left))
    ups.append(lax.ppermute(ups[1], "tp", right))
    down_even = lax.ppermute(downs[2][0:1], "tp", left)
    down_odd = lax.ppermute(downs[1][1:2], "tp", right)

    send, pick = call(
        lambda *refs: dispatch_kernel(experts, local_experts, quarter, *refs),
        (shape((groups * chunk, half), BF16), shape((2, slots, token_count), BF16)),
        (member, routing.T, gate_weights.T, tokens, cotangent),
        scalars=1,
    )
    landed = lax.all_to_all(
        send.reshape(groups, chunk, half), "ep", split_axis=0, concat_axis=0, tiled=True
    ).reshape(groups * chunk, half)

    from_left = lax.ppermute(landed, "tp", right)
    from_right = lax.ppermute(landed, "tp", left)
    middle = groups * chunk // 2
    opposite_low = lax.ppermute(from_right[:middle], "tp", left)
    opposite_high = lax.ppermute(from_left[middle:], "tp", right)

    back_rows = (local_experts * quarter + 1) * SUBLANES
    back = call(
        lambda *refs: input_kernel(local_experts, quarter, *refs),
        shape((groups * back_rows, LANES), F32),
        (landed, *gates, *ups, *downs, down_even, down_odd),
        scratch=[VMEM((own, model_width), BF16)] * 2,
    )
    back = back.astype(F16).reshape(groups, back_rows, LANES)
    back = lax.all_to_all(back, "ep", split_axis=0, concat_axis=0, tiled=True)
    back = back.astype(F32).reshape(groups * back_rows, LANES)
    count = token_count // members
    part = shape((count + SUBLANES, model_width), F32)
    mine, to_right, to_left, to_across = call(
        lambda *refs: combine_kernel(members, groups, *refs),
        (part,) * 4,
        (member, back, pick),
        scalars=1,
        scratch=[VMEM((token_count, model_width), F32)],
    )
    pieces = (
        lax.ppermute(to_right, "tp", right),
        lax.ppermute(to_left, "tp", left),
        lax.ppermute(to_across, "tp", across),
    )
    summed, gates_grad = call(
        sum_kernel,
        (shape((count, model_width), BF16), shape((top_count, token_count), F32)),
        (mine, *pieces, gate_weights.T),
    )
    pieces = (
        lax.ppermute(summed, "tp", right),
        lax.ppermute(summed, "tp", left),
        lax.ppermute(summed, "tp", across),
    )
    tokens_grad = call(
        lambda *refs: place_kernel(members, *refs),
        shape((token_count, model_width), BF16),
        (member, summed, *pieces),
        scalars=1,
    )

    gate_grad, up_grad, down_grad = call(
        lambda *refs: weight_kernel(local_experts, quarter, *refs),
        (
            shape((local_experts, model_width, hidden_width), F32),
            shape((local_experts, model_width, hidden_width), F32),
            shape((local_experts, hidden_width, model_width), F32),
        ),
        (landed, from_left, from_right, opposite_low, opposite_high, gate_proj, up_proj, down_proj),
        scratch=[VMEM((members * own, model_width), BF16)] * 2,
    )
    return (tokens_grad, gates_grad.T, gate_grad, up_grad, down_grad)


def solution(mesh):
    in_specs = (
        P("ep", None),
        P("ep", None),
        P("ep", None),
        P("ep", None),
        P("ep", None, "tp"),
        P("ep", None, "tp"),
        P("ep", "tp", None),
    )
    out_specs = (
        P("ep", None),
        P("ep", None),
        P("ep", None, "tp"),
        P("ep", None, "tp"),
        P("ep", "tp", None),
    )
    return jax.shard_map(step, mesh=mesh, in_specs=in_specs, out_specs=out_specs, check_vma=False)
```

```python
import jax
import jax.numpy as jnp
from jax import lax
from jax.experimental import pallas as pl
from jax.experimental.pallas import tpu as pltpu
from jax.sharding import PartitionSpec as P


F32 = jnp.float32
I16 = jnp.int16
BF16 = jnp.bfloat16
I32 = jnp.int32
LANES = 128
SUBLANES = 8
BLOCK = 16
PARTS = 4
TOP_CODE = 32766.0
STEPS = 8192.0
FINE = 32768.0
VMEM = pltpu.VMEM
SMEM = pltpu.SMEM
NN = ((1,), (0,))
NT = ((1,), (1,))
TN = ((0,), (0,))


def mm(a, b, dims=NN):
    return lax.dot_general(a, b, (dims, ((), ())), preferred_element_type=F32)


def iota(shape, dim):
    return lax.broadcasted_iota(I32, shape, dim)


def split3(value):
    high = value.astype(BF16)
    rest = value - high.astype(F32)
    middle = rest.astype(BF16)
    low = (rest - middle.astype(F32)).astype(BF16)
    return high, middle, low


def exponent(value):
    return jnp.floor(jnp.log(jnp.maximum(value, 1e-30)) * 1.4426950408889634)


def row_scale(power, steps):
    return steps * jnp.exp2(power) * (1.0 / (STEPS * TOP_CODE))


def code_rows(value):
    largest = jnp.maximum(jnp.max(jnp.abs(value), axis=1, keepdims=True), 1e-30)
    power = exponent(largest)
    steps = jnp.ceil(largest * jnp.exp2(-power) * STEPS)
    return jnp.round(value * (1.0 / row_scale(power, steps))), power, steps


def code_values(value):
    power = exponent(jnp.abs(value))
    value = value * jnp.exp2(-power) * STEPS
    coarse = jnp.round(value)
    return power, coarse, jnp.round((value - coarse) * FINE)


def decode_values(power, coarse, fine):
    return (coarse + fine * (1.0 / FINE)) * (jnp.exp2(power) * (1.0 / STEPS))


def to_code(value):
    return value.astype(I32).astype(I16)


def from_code(value):
    return value.astype(I32).astype(F32)


def slot_rows(experts, local_experts, quarter, member, routing):
    token_count = routing.shape[1]
    expert = iota((experts, token_count), 0)
    chosen = [routing[k : k + 1, :] for k in range(2)]
    onehot = [jnp.where(expert == c, 1.0, 0.0) for c in chosen]
    earlier = iota((token_count, token_count), 0)
    later = iota((token_count, token_count), 1)
    upper = jnp.where(earlier < later, 1.0, 0.0).astype(BF16)
    before = mm((onehot[0] + onehot[1]).astype(BF16), upper)
    places = []
    for k in range(2):
        position = jnp.sum(onehot[k] * before, axis=0, keepdims=True).astype(I32)
        local = position - member[0] * quarter
        present = (local >= 0) & (local < quarter)
        device = chosen[k] // local_experts
        places.append((present, device, (chosen[k] - device * local_experts) * quarter + local))
    return places


def picked(rows_out, source, places, group, weights=None):
    token_count = source.shape[0]
    row_count, part_width = rows_out.shape
    chunk = PARTS * group
    row = iota((row_count, token_count), 0)
    at = [jnp.where(present, device * chunk + within, -chunk) for present, device, within in places]
    total = None
    for part in range(PARTS):
        hits = [jnp.where(row == r + part * group, 1.0, 0.0) for r in at]
        values = source[:, part * part_width : (part + 1) * part_width]
        value = mm((hits[0] + hits[1]).astype(BF16), values)
        if weights is not None:
            weighted = hits[0] * weights[0:1, :] + hits[1] * weights[1:2, :]
            value = jnp.sum(weighted, axis=1, keepdims=True) * value
        total = value if total is None else total + value
    rows_out[...] = total.astype(BF16)


def token_kernel(experts, local_experts, quarter, member, routing, tokens, rows_out):
    places = slot_rows(experts, local_experts, quarter, member, routing)
    picked(rows_out, tokens, places, local_experts * quarter)


def scaled_kernel(
    experts, local_experts, quarter, member, routing, weights, cotangent, rows_out, pick
):
    places = slot_rows(experts, local_experts, quarter, member, routing)
    picked(rows_out, cotangent, places, local_experts * quarter, weights)
    slot = iota(pick.shape[1:], 0)
    devices = experts // local_experts
    for k, (present, device, within) in enumerate(places):
        wanted = jnp.where(present, within * devices + device, -1)
        pick[k] = jnp.where(slot == wanted, 1.0, 0.0).astype(BF16)


def land(source, expert, local_experts, quarter, rows, offset):
    part_width = source.shape[1]
    group = local_experts * quarter
    chunk = PARTS * group
    out_rows = BLOCK * quarter
    index = iota((PARTS * out_rows, 1), 0)
    part = index // out_rows
    rest = index - part * out_rows
    slot = rest // BLOCK
    wanted = (rest - slot * BLOCK) * chunk + part * group + expert * quarter + slot
    column = iota((PARTS * out_rows, BLOCK * chunk), 1)
    permutation = jnp.where(column == wanted, 1.0, 0.0).astype(BF16)
    for block in range(source.shape[0] // (BLOCK * chunk)):
        moved = mm(permutation, source[block * BLOCK * chunk : (block + 1) * BLOCK * chunk, :])
        moved = moved.astype(BF16)
        at = offset + block * out_rows
        for p in range(PARTS):
            columns = slice(p * part_width, (p + 1) * part_width)
            rows[at : at + out_rows, columns] = moved[p * out_rows : (p + 1) * out_rows]


def hidden_terms(gate_pre, up_pre, hidden_grad):
    gate_pre = gate_pre.astype(BF16).astype(F32)
    up_pre = up_pre.astype(BF16).astype(F32)
    sigmoid = jax.nn.sigmoid(gate_pre)
    activated = gate_pre * sigmoid
    hidden = activated * up_pre
    gate_grad = (hidden_grad * up_pre * sigmoid * (1.0 + gate_pre * (1.0 - sigmoid))).astype(BF16)
    up_grad = (hidden_grad * activated).astype(BF16)
    return hidden, gate_grad, up_grad


def input_kernel(local_experts, quarter, landed_rows, landed_scaled, *refs):
    gates, ups, downs = refs[0:4], refs[4:8], refs[8:11]
    down_even, down_odd, out, rows, scaled, coded = refs[11:]
    own, _ = rows.shape
    slots = local_experts * quarter
    devices = own // quarter
    stride = (slots + 1) * SUBLANES
    for i in range(slots, SUBLANES):
        at = slots * SUBLANES + i
        coded[pl.ds(at, devices, stride=stride), :] = jnp.zeros((devices, LANES), F32)
    for expert in range(local_experts):
        land(landed_rows, expert, local_experts, quarter, rows, 0)
        land(landed_scaled, expert, local_experts, quarter, scaled, 0)
        gate = jnp.concatenate([g[expert] for g in gates], axis=1)
        up = jnp.concatenate([u[expert] for u in ups], axis=1)
        last = (down_even, down_odd)[expert][0]
        down = jnp.concatenate([d[expert] for d in downs] + [last], axis=0)
        hidden_grad = mm(scaled[...], down, NT)
        hidden, gate_grad, up_grad = hidden_terms(mm(rows[...], gate), mm(rows[...], up), hidden_grad)
        product = jnp.sum(hidden_grad * hidden, axis=1, keepdims=True)
        grad = mm(gate_grad, gate, NT) + mm(up_grad, up, NT)
        grad, power, steps = code_rows(grad)
        lane = iota((own, LANES), 1)
        tail = jnp.zeros((own, LANES), F32)
        for at, column in enumerate((power, steps) + code_values(product)):
            tail = jnp.where(lane == at, column, tail)
        for block in range(devices // BLOCK):
            for q in range(quarter):
                at = (block * quarter + q) * BLOCK
                to = block * BLOCK * stride
                slot = expert * quarter + q
                for i in range(SUBLANES):
                    piece = grad[at : at + BLOCK, i * LANES : (i + 1) * LANES]
                    coded[pl.ds(to + slot * SUBLANES + i, BLOCK, stride=stride), :] = piece
                to += slots * SUBLANES + slot
                coded[pl.ds(to, BLOCK, stride=stride), :] = tail[at : at + BLOCK]
    out[...] = to_code(coded[...])


def weight_kernel(local_experts, quarter, *refs):
    (gate, up, down), (gate_out, up_out, down_out), (rows, scaled) = refs[8:11], refs[11:14], refs[14:]
    own = rows.shape[0] // 4
    hidden_width = gate.shape[2]

    def one(expert, carry):
        for i in range(4):
            land(refs[i], expert, local_experts, quarter, rows, i * own)
            land(refs[4 + i], expert, local_experts, quarter, scaled, i * own)
        both = mm(rows[...], jnp.concatenate([gate[expert], up[expert]], axis=1))
        hidden_grad = mm(scaled[...], down[expert], NT)
        hidden, gate_grad, up_grad = hidden_terms(
            both[:, :hidden_width], both[:, hidden_width:], hidden_grad
        )
        grads = mm(rows[...], jnp.concatenate([gate_grad, up_grad], axis=1), TN)
        gate_out[expert] = grads[:, :hidden_width]
        up_out[expert] = grads[:, hidden_width:]
        down_out[expert] = mm(hidden.astype(BF16), scaled[...], TN)
        return carry

    lax.fori_loop(0, local_experts, one, 0)


def member_rows(member, distance, members, count):
    return pl.ds(pl.multiple_of(lax.rem(member + distance, members) * count, count), count)


def combine_kernel(members, devices, member, coded, pick, *refs):
    outs, total, back = refs[:-2], refs[-2], refs[-1]
    back[...] = from_code(coded[...])
    token_count, tail_width = total.shape
    width = tail_width - LANES
    slots = pick.shape[1] // devices
    stride = (slots + 1) * SUBLANES
    tails = [
        back[pl.ds(slots * SUBLANES + slot, devices, stride=stride), :] for slot in range(slots)
    ]
    tail = jnp.concatenate(tails, axis=0)
    scale = row_scale(tail[:, 0:1], tail[:, 1:2])
    columns = []
    for i in range(SUBLANES):
        pieces = [
            back[pl.ds(slot * SUBLANES + i, devices, stride=stride), :] for slot in range(slots)
        ]
        columns.append(jnp.concatenate(pieces, axis=0))
    grad = jnp.concatenate(columns, axis=1) * scale
    both = pick[0] + pick[1]
    grad, power, steps = code_rows(sum(mm(both, part, TN) for part in split3(grad)))
    total[:, 0:width] = grad
    lane = iota((token_count, LANES), 1)
    total[:, width:] = jnp.where(lane == 0, power, jnp.where(lane == 1, steps, 0.0))
    product = decode_values(tail[:, 2:3], tail[:, 3:4], tail[:, 4:5])
    sums = [jnp.sum(pick[k].astype(F32) * product, axis=0, keepdims=True) for k in range(2)]
    power, coarse, fine = code_values(jnp.concatenate(sums, axis=1))
    spare = jnp.zeros((1, tail_width - 4 * token_count), F32)
    first = jnp.concatenate([power, coarse, spare], axis=1)
    second = jnp.concatenate([fine, jnp.zeros_like(fine), spare], axis=1)
    line = iota((SUBLANES, tail_width), 0)
    lines = to_code(jnp.where(line == 0, first, jnp.where(line == 1, second, 0.0)))
    count = token_count // members
    for out, distance in zip(outs, (0, 1, 3, 2)):
        out[0:count, :] = to_code(total[member_rows(member[0], distance, members, count), :])
        out[count : count + SUBLANES, :] = lines


def sum_kernel(own, from_left, from_right, from_opposite, weights, grad_out, gates_out):
    count, width = grad_out.shape
    token_count = weights.shape[1]
    parts = [from_code(part[...]) for part in (own, from_left, from_right, from_opposite)]
    grads = [
        part[:count, :width] * row_scale(part[:count, width : width + 1], part[:count, width + 1 : width + 2])
        for part in parts
    ]
    grad_out[...] = ((grads[0] + grads[3]) + (grads[1] + grads[2])).astype(BF16)
    values = 2 * token_count
    products = [
        decode_values(
            part[count : count + 1, 0:values],
            part[count : count + 1, values : 2 * values],
            part[count + 1 : count + 2, 0:values],
        )
        for part in parts
    ]
    product = (products[0] + products[3]) + (products[1] + products[2])
    for k in range(2):
        gates_out[k : k + 1, :] = product[:, k * token_count : (k + 1) * token_count] / weights[k : k + 1, :]


def place_kernel(members, member, own, from_left, from_right, from_opposite, out):
    count = own.shape[0]
    for piece, distance in ((own, 0), (from_left, 3), (from_right, 1), (from_opposite, 2)):
        out[member_rows(member[0], distance, members, count), :] = piece[...]


def step(tokens, cotangent, routing, gate_weights, gate_proj, up_proj, down_proj):
    token_count, model_width = tokens.shape
    top_count = routing.shape[1]
    local_experts, _, hidden_width = gate_proj.shape
    groups = lax.axis_size("ep")
    members = lax.axis_size("tp")
    experts = local_experts * groups
    capacity = members * (
        (3 * token_count * top_count + experts * members - 1) // (experts * members)
    )
    quarter = capacity // members
    slots = experts * quarter
    own = groups * quarter
    chunk = PARTS * local_experts * quarter
    part_width = model_width // PARTS
    member = lax.axis_index("tp").astype(I32).reshape(1)
    right = [(i, (i + 1) % members) for i in range(members)]
    left = [(i, (i - 1) % members) for i in range(members)]
    across = [(i, (i + 2) % members) for i in range(members)]
    whole = pl.BlockSpec(memory_space=VMEM)
    scalar = pl.BlockSpec(memory_space=SMEM)

    def call(kernel, out_shape, args, scalars=0, scratch=()):
        return pl.pallas_call(
            kernel,
            out_shape=out_shape,
            in_specs=[scalar] * scalars + [whole] * (len(args) - scalars),
            out_specs=jax.tree.map(lambda _: whole, out_shape),
            scratch_shapes=list(scratch),
        )(*args)

    def shape(dims, dtype):
        return jax.ShapeDtypeStruct(dims, dtype)

    gates, ups, downs = [gate_proj], [up_proj], [down_proj]
    for kept, mine in ((gates, gate_proj), (ups, up_proj), (downs, down_proj)):
        kept.append(lax.ppermute(mine, "tp", right))
        kept.append(lax.ppermute(mine, "tp", left))
    gates.append(lax.ppermute(gates[2], "tp", left))
    ups.append(lax.ppermute(ups[1], "tp", right))
    down_even = lax.ppermute(downs[2][0:1], "tp", left)
    down_odd = lax.ppermute(downs[1][1:2], "tp", right)

    sizes = (experts, local_experts, quarter)
    send_shape = shape((groups * chunk, part_width), BF16)

    def to_experts(send):
        send = send.reshape(groups, chunk, part_width)
        landed = lax.all_to_all(send, "ep", split_axis=0, concat_axis=0, tiled=True)
        return landed.reshape(groups * chunk, part_width)

    def swap(landed):
        return [landed, lax.ppermute(landed, "tp", right), lax.ppermute(landed, "tp", left)]

    send = call(
        lambda *refs: token_kernel(*sizes, *refs),
        send_shape,
        (member, routing.T, tokens),
        scalars=1,
    )
    rows = to_experts(send)
    send, pick = call(
        lambda *refs: scaled_kernel(*sizes, *refs),
        (send_shape, shape((2, slots, token_count), BF16)),
        (member, routing.T, gate_weights.T, cotangent),
        scalars=1,
    )
    scaled = to_experts(send)
    rows = swap(rows)
    scaled = swap(scaled)
    rows.append(lax.ppermute(rows[2], "tp", left))
    scaled.append(lax.ppermute(scaled[1], "tp", right))

    back_rows = (local_experts * quarter + 1) * SUBLANES
    back = call(
        lambda *refs: input_kernel(local_experts, quarter, *refs),
        shape((groups * back_rows, LANES), I16),
        (rows[0], scaled[0], *gates, *ups, *downs, down_even, down_odd),
        scratch=[VMEM((own, model_width), BF16)] * 2 + [VMEM((groups * back_rows, LANES), F32)],
    )
    back = back.reshape(groups, back_rows, LANES)
    back = lax.all_to_all(back, "ep", split_axis=0, concat_axis=0, tiled=True)
    back = back.reshape(groups * back_rows, LANES)
    count = token_count // members
    tail_width = model_width + LANES
    part = shape((count + SUBLANES, tail_width), I16)
    mine, to_right, to_left, to_across = call(
        lambda *refs: combine_kernel(members, groups, *refs),
        (part,) * 4,
        (member, back, pick),
        scalars=1,
        scratch=[VMEM((token_count, tail_width), F32), VMEM((groups * back_rows, LANES), F32)],
    )
    pieces = (
        lax.ppermute(to_right, "tp", right),
        lax.ppermute(to_left, "tp", left),
        lax.ppermute(to_across, "tp", across),
    )
    summed, gates_grad = call(
        sum_kernel,
        (shape((count, model_width), BF16), shape((top_count, token_count), F32)),
        (mine, *pieces, gate_weights.T),
    )
    pieces = (
        lax.ppermute(summed, "tp", right),
        lax.ppermute(summed, "tp", left),
        lax.ppermute(summed, "tp", across),
    )
    tokens_grad = call(
        lambda *refs: place_kernel(members, *refs),
        shape((token_count, model_width), BF16),
        (member, summed, *pieces),
        scalars=1,
    )

    gate_grad, up_grad, down_grad = call(
        lambda *refs: weight_kernel(local_experts, quarter, *refs),
        (
            shape((local_experts, model_width, hidden_width), F32),
            shape((local_experts, model_width, hidden_width), F32),
            shape((local_experts, hidden_width, model_width), F32),
        ),
        (*rows, *scaled, gate_proj, up_proj, down_proj),
        scratch=[VMEM((members * own, model_width), BF16)] * 2,
    )
    return (tokens_grad, gates_grad.T, gate_grad, up_grad, down_grad)


def solution(mesh):
    in_specs = (
        P("ep", None),
        P("ep", None),
        P("ep", None),
        P("ep", None),
        P("ep", None, "tp"),
        P("ep", None, "tp"),
        P("ep", "tp", None),
    )
    out_specs = (
        P("ep", None),
        P("ep", None),
        P("ep", None, "tp"),
        P("ep", None, "tp"),
        P("ep", "tp", None),
    )
    return jax.shard_map(step, mesh=mesh, in_specs=in_specs, out_specs=out_specs, check_vma=False)
```

```python
import jax
import jax.numpy as jnp
from jax import lax
from jax.experimental import pallas as pl
from jax.experimental.pallas import tpu as pltpu
from jax.sharding import PartitionSpec as P


F32 = jnp.float32
I16 = jnp.int16
BF16 = jnp.bfloat16
I32 = jnp.int32
LANES = 128
SUBLANES = 8
BLOCK = 16
HALVES = 2
TOP_CODE = 32766.0
STEPS = 8192.0
FINE = 32768.0
VMEM = pltpu.VMEM
SMEM = pltpu.SMEM
NN = ((1,), (0,))
NT = ((1,), (1,))
TN = ((0,), (0,))


def mm(a, b, dims=NN):
    return lax.dot_general(a, b, (dims, ((), ())), preferred_element_type=F32)


def iota(shape, dim):
    return lax.broadcasted_iota(I32, shape, dim)


def split3(value):
    high = value.astype(BF16)
    rest = value - high.astype(F32)
    middle = rest.astype(BF16)
    low = (rest - middle.astype(F32)).astype(BF16)
    return high, middle, low


def exponent(value):
    return jnp.floor(jnp.log(jnp.maximum(value, 1e-30)) * 1.4426950408889634)


def row_scale(power, steps):
    return steps * jnp.exp2(power) * (1.0 / (STEPS * TOP_CODE))


def code_rows(value):
    largest = jnp.maximum(jnp.max(jnp.abs(value), axis=1, keepdims=True), 1e-30)
    power = exponent(largest)
    steps = jnp.ceil(largest * jnp.exp2(-power) * STEPS)
    return jnp.round(value * (1.0 / row_scale(power, steps))), power, steps


def code_values(value):
    power = exponent(jnp.abs(value))
    value = value * jnp.exp2(-power) * STEPS
    coarse = jnp.round(value)
    return power, coarse, jnp.round((value - coarse) * FINE)


def decode_values(power, coarse, fine):
    return (coarse + fine * (1.0 / FINE)) * (jnp.exp2(power) * (1.0 / STEPS))


def to_code(value):
    return value.astype(I32).astype(I16)


def from_code(value):
    return value.astype(I32).astype(F32)


def dispatch_kernel(
    experts, local_experts, quarter, member, routing, weights, tokens, cotangent, rows_out, pick
):
    token_count, width = tokens.shape
    half = width // HALVES
    row_count = rows_out.shape[0]
    slots = pick.shape[1]
    group = local_experts * quarter
    chunk = HALVES * 2 * group
    devices = experts // local_experts
    expert = iota((experts, token_count), 0)
    chosen = [routing[k : k + 1, :] for k in range(2)]
    onehot = [jnp.where(expert == c, 1.0, 0.0) for c in chosen]
    earlier = iota((token_count, token_count), 0)
    later = iota((token_count, token_count), 1)
    upper = jnp.where(earlier < later, 1.0, 0.0).astype(BF16)
    before = mm((onehot[0] + onehot[1]).astype(BF16), upper)
    row = iota((row_count, token_count), 0)
    slot = iota((slots, token_count), 0)
    token_rows = []
    for k in range(2):
        position = jnp.sum(onehot[k] * before, axis=0, keepdims=True).astype(I32)
        local = position - member[0] * quarter
        present = (local >= 0) & (local < quarter)
        device = chosen[k] // local_experts
        within = (chosen[k] - device * local_experts) * quarter + local
        pick[k] = jnp.where(slot == jnp.where(present, within * devices + device, -1), 1.0, 0.0).astype(BF16)
        token_rows.append(jnp.where(present, device * chunk + within, -chunk))
    total = None
    for h in range(HALVES):
        columns = slice(h * half, (h + 1) * half)
        base = h * 2 * group
        hits = [row == r + base for r in token_rows]
        part = mm(jnp.where(hits[0] | hits[1], 1.0, 0.0).astype(BF16), tokens[:, columns])
        hits = [row == r + (base + group) for r in token_rows]
        weighted = jnp.where(hits[0], weights[0:1, :], jnp.where(hits[1], weights[1:2, :], 0.0))
        slot_weight = jnp.sum(weighted, axis=1, keepdims=True)
        chosen_rows = jnp.where(hits[0] | hits[1], 1.0, 0.0).astype(BF16)
        part = part + slot_weight * mm(chosen_rows, cotangent[:, columns])
        total = part if total is None else total + part
    rows_out[...] = total.astype(BF16)


def land(source, expert, local_experts, quarter, rows, scaled, offset):
    half = source.shape[1]
    group = local_experts * quarter
    chunk = HALVES * 2 * group
    out_rows = BLOCK * quarter
    index = iota((HALVES * 2 * out_rows, 1), 0)
    kind = index // out_rows
    rest = index - kind * out_rows
    slot = rest // BLOCK
    wanted = (rest - slot * BLOCK) * chunk + kind * group + expert * quarter + slot
    column = iota((HALVES * 2 * out_rows, BLOCK * chunk), 1)
    permutation = jnp.where(column == wanted, 1.0, 0.0).astype(BF16)
    for block in range(source.shape[0] // (BLOCK * chunk)):
        moved = mm(permutation, source[block * BLOCK * chunk : (block + 1) * BLOCK * chunk, :])
        moved = moved.astype(BF16)
        at = slice(offset + block * out_rows, offset + (block + 1) * out_rows)
        for h in range(HALVES):
            columns = slice(h * half, (h + 1) * half)
            first = 2 * h * out_rows
            rows[at, columns] = moved[first : first + out_rows]
            scaled[at, columns] = moved[first + out_rows : first + 2 * out_rows]


def hidden_terms(gate_pre, up_pre, hidden_grad):
    gate_pre = gate_pre.astype(BF16).astype(F32)
    up_pre = up_pre.astype(BF16).astype(F32)
    sigmoid = jax.nn.sigmoid(gate_pre)
    activated = gate_pre * sigmoid
    hidden = activated * up_pre
    gate_grad = (hidden_grad * up_pre * sigmoid * (1.0 + gate_pre * (1.0 - sigmoid))).astype(BF16)
    up_grad = (hidden_grad * activated).astype(BF16)
    return hidden, gate_grad, up_grad


def input_kernel(local_experts, quarter, landed, *refs):
    gates, ups, downs = refs[0:4], refs[4:8], refs[8:11]
    down_even, down_odd, out, rows, scaled, coded = refs[11:]
    own, _ = rows.shape
    slots = local_experts * quarter
    devices = own // quarter
    stride = (slots + 1) * SUBLANES
    for i in range(slots, SUBLANES):
        at = slots * SUBLANES + i
        coded[pl.ds(at, devices, stride=stride), :] = jnp.zeros((devices, LANES), F32)
    for expert in range(local_experts):
        land(landed, expert, local_experts, quarter, rows, scaled, 0)
        gate = jnp.concatenate([g[expert] for g in gates], axis=1)
        up = jnp.concatenate([u[expert] for u in ups], axis=1)
        last = (down_even, down_odd)[expert][0]
        down = jnp.concatenate([d[expert] for d in downs] + [last], axis=0)
        hidden_grad = mm(scaled[...], down, NT)
        hidden, gate_grad, up_grad = hidden_terms(mm(rows[...], gate), mm(rows[...], up), hidden_grad)
        product = jnp.sum(hidden_grad * hidden, axis=1, keepdims=True)
        grad = mm(gate_grad, gate, NT) + mm(up_grad, up, NT)
        grad, power, steps = code_rows(grad)
        lane = iota((own, LANES), 1)
        tail = jnp.zeros((own, LANES), F32)
        for at, column in enumerate((power, steps) + code_values(product)):
            tail = jnp.where(lane == at, column, tail)
        for block in range(devices // BLOCK):
            for q in range(quarter):
                at = (block * quarter + q) * BLOCK
                to = block * BLOCK * stride
                slot = expert * quarter + q
                for i in range(SUBLANES):
                    piece = grad[at : at + BLOCK, i * LANES : (i + 1) * LANES]
                    coded[pl.ds(to + slot * SUBLANES + i, BLOCK, stride=stride), :] = piece
                to += slots * SUBLANES + slot
                coded[pl.ds(to, BLOCK, stride=stride), :] = tail[at : at + BLOCK]
    out[...] = to_code(coded[...])


def weight_kernel(local_experts, quarter, *refs):
    sources, (gate, up, down), (gate_out, up_out, down_out) = refs[0:5], refs[5:8], refs[8:11]
    rows, scaled = refs[11:]
    chunk = HALVES * 2 * local_experts * quarter
    hidden_width = gate.shape[2]

    def one(expert, carry):
        offset = 0
        for source in sources:
            land(source, expert, local_experts, quarter, rows, scaled, offset)
            offset += source.shape[0] // chunk * quarter
        both = mm(rows[...], jnp.concatenate([gate[expert], up[expert]], axis=1))
        hidden_grad = mm(scaled[...], down[expert], NT)
        hidden, gate_grad, up_grad = hidden_terms(
            both[:, :hidden_width], both[:, hidden_width:], hidden_grad
        )
        grads = mm(rows[...], jnp.concatenate([gate_grad, up_grad], axis=1), TN)
        gate_out[expert] = grads[:, :hidden_width]
        up_out[expert] = grads[:, hidden_width:]
        down_out[expert] = mm(hidden.astype(BF16), scaled[...], TN)
        return carry

    lax.fori_loop(0, local_experts, one, 0)


def member_rows(member, distance, members, count):
    return pl.ds(pl.multiple_of(lax.rem(member + distance, members) * count, count), count)


def combine_kernel(members, devices, member, coded, pick, *refs):
    outs, total, back = refs[:-2], refs[-2], refs[-1]
    back[...] = from_code(coded[...])
    token_count, tail_width = total.shape
    width = tail_width - LANES
    slots = pick.shape[1] // devices
    stride = (slots + 1) * SUBLANES
    tails = [
        back[pl.ds(slots * SUBLANES + slot, devices, stride=stride), :] for slot in range(slots)
    ]
    tail = jnp.concatenate(tails, axis=0)
    scale = row_scale(tail[:, 0:1], tail[:, 1:2])
    columns = []
    for i in range(SUBLANES):
        pieces = [
            back[pl.ds(slot * SUBLANES + i, devices, stride=stride), :] for slot in range(slots)
        ]
        columns.append(jnp.concatenate(pieces, axis=0))
    grad = jnp.concatenate(columns, axis=1) * scale
    both = pick[0] + pick[1]
    grad, power, steps = code_rows(sum(mm(both, part, TN) for part in split3(grad)))
    total[:, 0:width] = grad
    lane = iota((token_count, LANES), 1)
    total[:, width:] = jnp.where(lane == 0, power, jnp.where(lane == 1, steps, 0.0))
    product = decode_values(tail[:, 2:3], tail[:, 3:4], tail[:, 4:5])
    sums = [jnp.sum(pick[k].astype(F32) * product, axis=0, keepdims=True) for k in range(2)]
    power, coarse, fine = code_values(jnp.concatenate(sums, axis=1))
    spare = jnp.zeros((1, tail_width - 4 * token_count), F32)
    first = jnp.concatenate([power, coarse, spare], axis=1)
    second = jnp.concatenate([fine, jnp.zeros_like(fine), spare], axis=1)
    line = iota((SUBLANES, tail_width), 0)
    lines = to_code(jnp.where(line == 0, first, jnp.where(line == 1, second, 0.0)))
    count = token_count // members
    for out, distance in zip(outs, (0, 1, 3, 2)):
        out[0:count, :] = to_code(total[member_rows(member[0], distance, members, count), :])
        out[count : count + SUBLANES, :] = lines


def sum_kernel(own, from_left, from_right, from_opposite, weights, grad_out, gates_out):
    count, width = grad_out.shape
    token_count = weights.shape[1]
    parts = [from_code(part[...]) for part in (own, from_left, from_right, from_opposite)]
    grads = [
        part[:count, :width] * row_scale(part[:count, width : width + 1], part[:count, width + 1 : width + 2])
        for part in parts
    ]
    grad_out[...] = ((grads[0] + grads[3]) + (grads[1] + grads[2])).astype(BF16)
    values = 2 * token_count
    products = [
        decode_values(
            part[count : count + 1, 0:values],
            part[count : count + 1, values : 2 * values],
            part[count + 1 : count + 2, 0:values],
        )
        for part in parts
    ]
    product = (products[0] + products[3]) + (products[1] + products[2])
    for k in range(2):
        gates_out[k : k + 1, :] = product[:, k * token_count : (k + 1) * token_count] / weights[k : k + 1, :]


def place_kernel(members, member, own, from_left, from_right, from_opposite, out, sems):
    count = own.shape[0]
    copies = []
    for piece, distance in ((own, 0), (from_left, 3), (from_right, 1), (from_opposite, 2)):
        to = out.at[member_rows(member[0], distance, members, count), :]
        copies.append(pltpu.make_async_copy(piece, to, sems.at[distance]))
        copies[-1].start()
    for copy in copies:
        copy.wait()


def step(tokens, cotangent, routing, gate_weights, gate_proj, up_proj, down_proj):
    token_count, model_width = tokens.shape
    top_count = routing.shape[1]
    local_experts, _, hidden_width = gate_proj.shape
    groups = lax.axis_size("ep")
    members = lax.axis_size("tp")
    experts = local_experts * groups
    capacity = members * (
        (3 * token_count * top_count + experts * members - 1) // (experts * members)
    )
    quarter = capacity // members
    slots = experts * quarter
    own = groups * quarter
    chunk = HALVES * 2 * local_experts * quarter
    half = model_width // HALVES
    member = lax.axis_index("tp").astype(I32).reshape(1)
    right = [(i, (i + 1) % members) for i in range(members)]
    left = [(i, (i - 1) % members) for i in range(members)]
    across = [(i, (i + 2) % members) for i in range(members)]
    whole = pl.BlockSpec(memory_space=VMEM)
    scalar = pl.BlockSpec(memory_space=SMEM)

    def call(kernel, out_shape, args, scalars=0, scratch=()):
        return pl.pallas_call(
            kernel,
            out_shape=out_shape,
            in_specs=[scalar] * scalars + [whole] * (len(args) - scalars),
            out_specs=jax.tree.map(lambda _: whole, out_shape),
            scratch_shapes=list(scratch),
        )(*args)

    def shape(dims, dtype):
        return jax.ShapeDtypeStruct(dims, dtype)

    gates, ups, downs = [gate_proj], [up_proj], [down_proj]
    for kept, mine in ((gates, gate_proj), (ups, up_proj), (downs, down_proj)):
        kept.append(lax.ppermute(mine, "tp", right))
        kept.append(lax.ppermute(mine, "tp", left))
    gates.append(lax.ppermute(gates[2], "tp", left))
    ups.append(lax.ppermute(ups[1], "tp", right))
    down_even = lax.ppermute(downs[2][0:1], "tp", left)
    down_odd = lax.ppermute(downs[1][1:2], "tp", right)

    send, pick = call(
        lambda *refs: dispatch_kernel(experts, local_experts, quarter, *refs),
        (shape((groups * chunk, half), BF16), shape((2, slots, token_count), BF16)),
        (member, routing.T, gate_weights.T, tokens, cotangent),
        scalars=1,
    )
    landed = lax.all_to_all(
        send.reshape(groups, chunk, half), "ep", split_axis=0, concat_axis=0, tiled=True
    ).reshape(groups * chunk, half)

    from_left = lax.ppermute(landed, "tp", right)
    from_right = lax.ppermute(landed, "tp", left)
    middle = groups * chunk // 2
    opposite_low = lax.ppermute(from_right[:middle], "tp", left)
    opposite_high = lax.ppermute(from_left[middle:], "tp", right)

    back_rows = (local_experts * quarter + 1) * SUBLANES
    back = call(
        lambda *refs: input_kernel(local_experts, quarter, *refs),
        shape((groups * back_rows, LANES), I16),
        (landed, *gates, *ups, *downs, down_even, down_odd),
        scratch=[VMEM((own, model_width), BF16)] * 2 + [VMEM((groups * back_rows, LANES), F32)],
    )
    back = back.reshape(groups, back_rows, LANES)
    back = lax.all_to_all(back, "ep", split_axis=0, concat_axis=0, tiled=True)
    back = back.reshape(groups * back_rows, LANES)
    count = token_count // members
    tail_width = model_width + LANES
    part = shape((count + SUBLANES, tail_width), I16)
    mine, to_right, to_left, to_across = call(
        lambda *refs: combine_kernel(members, groups, *refs),
        (part,) * 4,
        (member, back, pick),
        scalars=1,
        scratch=[VMEM((token_count, tail_width), F32), VMEM((groups * back_rows, LANES), F32)],
    )
    pieces = (
        lax.ppermute(to_right, "tp", right),
        lax.ppermute(to_left, "tp", left),
        lax.ppermute(to_across, "tp", across),
    )
    summed, gates_grad = call(
        sum_kernel,
        (shape((count, model_width), BF16), shape((top_count, token_count), F32)),
        (mine, *pieces, gate_weights.T),
    )
    pieces = (
        lax.ppermute(summed, "tp", right),
        lax.ppermute(summed, "tp", left),
        lax.ppermute(summed, "tp", across),
    )
    anywhere = pl.BlockSpec(memory_space=pl.ANY)
    tokens_grad = pl.pallas_call(
        lambda *refs: place_kernel(members, *refs),
        out_shape=shape((token_count, model_width), BF16),
        in_specs=[scalar] + [anywhere] * 4,
        out_specs=anywhere,
        scratch_shapes=[pltpu.SemaphoreType.DMA((4,))],
        name="place",
    )(member, summed, *pieces)

    gate_grad, up_grad, down_grad = call(
        lambda *refs: weight_kernel(local_experts, quarter, *refs),
        (
            shape((local_experts, model_width, hidden_width), F32),
            shape((local_experts, model_width, hidden_width), F32),
            shape((local_experts, hidden_width, model_width), F32),
        ),
        (landed, from_left, from_right, opposite_low, opposite_high, gate_proj, up_proj, down_proj),
        scratch=[VMEM((members * own, model_width), BF16)] * 2,
    )
    return (tokens_grad, gates_grad.T, gate_grad, up_grad, down_grad)


def solution(mesh):
    in_specs = (
        P("ep", None),
        P("ep", None),
        P("ep", None),
        P("ep", None),
        P("ep", None, "tp"),
        P("ep", None, "tp"),
        P("ep", "tp", None),
    )
    out_specs = (
        P("ep", None),
        P("ep", None),
        P("ep", None, "tp"),
        P("ep", None, "tp"),
        P("ep", "tp", None),
    )
    return jax.shard_map(step, mesh=mesh, in_specs=in_specs, out_specs=out_specs, check_vma=False)
```

```python
import jax
import jax.numpy as jnp
from jax import lax
from jax.experimental import pallas as pl
from jax.experimental.pallas import tpu as pltpu
from jax.sharding import PartitionSpec as P


F32 = jnp.float32
I16 = jnp.int16
BF16 = jnp.bfloat16
I32 = jnp.int32
LANES = 128
SUBLANES = 8
BLOCK = 16
HALVES = 2
TOP_CODE = 32766.0
STEPS = 8192.0
FINE = 32768.0
VMEM = pltpu.VMEM
SMEM = pltpu.SMEM
NN = ((1,), (0,))
NT = ((1,), (1,))
TN = ((0,), (0,))


def mm(a, b, dims=NN):
    return lax.dot_general(a, b, (dims, ((), ())), preferred_element_type=F32)


def iota(shape, dim):
    return lax.broadcasted_iota(I32, shape, dim)


def split3(value):
    high = value.astype(BF16)
    rest = value - high.astype(F32)
    middle = rest.astype(BF16)
    low = (rest - middle.astype(F32)).astype(BF16)
    return high, middle, low


def exponent(value):
    return jnp.floor(jnp.log(jnp.maximum(value, 1e-30)) * 1.4426950408889634)


def row_scale(power, steps):
    return steps * jnp.exp2(power) * (1.0 / (STEPS * TOP_CODE))


def code_rows(value):
    largest = jnp.maximum(jnp.max(jnp.abs(value), axis=1, keepdims=True), 1e-30)
    power = exponent(largest)
    steps = jnp.ceil(largest * jnp.exp2(-power) * STEPS)
    return jnp.round(value * (1.0 / row_scale(power, steps))), power, steps


def code_values(value):
    power = exponent(jnp.abs(value))
    value = value * jnp.exp2(-power) * STEPS
    coarse = jnp.round(value)
    return power, coarse, jnp.round((value - coarse) * FINE)


def decode_values(power, coarse, fine):
    return (coarse + fine * (1.0 / FINE)) * (jnp.exp2(power) * (1.0 / STEPS))


def to_code(value):
    return value.astype(I32).astype(I16)


def from_code(value):
    return value.astype(I32).astype(F32)


def dispatch_kernel(
    experts, local_experts, quarter, member, routing, weights, tokens, cotangent, rows_out, pick
):
    token_count, width = tokens.shape
    half = width // HALVES
    row_count = rows_out.shape[0]
    slots = pick.shape[1]
    group = local_experts * quarter
    chunk = HALVES * 2 * group
    devices = experts // local_experts
    expert = iota((experts, token_count), 0)
    chosen = [routing[k : k + 1, :] for k in range(2)]
    onehot = [jnp.where(expert == c, 1.0, 0.0) for c in chosen]
    earlier = iota((token_count, token_count), 0)
    later = iota((token_count, token_count), 1)
    upper = jnp.where(earlier < later, 1.0, 0.0).astype(BF16)
    before = mm((onehot[0] + onehot[1]).astype(BF16), upper)
    row = iota((row_count, token_count), 0)
    slot = iota((slots, token_count), 0)
    token_rows = []
    for k in range(2):
        position = jnp.sum(onehot[k] * before, axis=0, keepdims=True).astype(I32)
        local = position - member[0] * quarter
        present = (local >= 0) & (local < quarter)
        device = chosen[k] // local_experts
        within = (chosen[k] - device * local_experts) * quarter + local
        pick[k] = jnp.where(slot == jnp.where(present, within * devices + device, -1), 1.0, 0.0).astype(BF16)
        token_rows.append(jnp.where(present, device * chunk + within, -chunk))
    total = None
    for h in range(HALVES):
        columns = slice(h * half, (h + 1) * half)
        base = h * 2 * group
        hits = [row == r + base for r in token_rows]
        part = mm(jnp.where(hits[0] | hits[1], 1.0, 0.0).astype(BF16), tokens[:, columns])
        hits = [row == r + (base + group) for r in token_rows]
        weighted = jnp.where(hits[0], weights[0:1, :], jnp.where(hits[1], weights[1:2, :], 0.0))
        slot_weight = jnp.sum(weighted, axis=1, keepdims=True)
        chosen_rows = jnp.where(hits[0] | hits[1], 1.0, 0.0).astype(BF16)
        part = part + slot_weight * mm(chosen_rows, cotangent[:, columns])
        total = part if total is None else total + part
    rows_out[...] = total.astype(BF16)


def land(source, expert, local_experts, quarter, rows, scaled, offset):
    half = source.shape[1]
    group = local_experts * quarter
    chunk = HALVES * 2 * group
    out_rows = BLOCK * quarter
    index = iota((HALVES * 2 * out_rows, 1), 0)
    kind = index // out_rows
    rest = index - kind * out_rows
    slot = rest // BLOCK
    wanted = (rest - slot * BLOCK) * chunk + kind * group + expert * quarter + slot
    column = iota((HALVES * 2 * out_rows, BLOCK * chunk), 1)
    permutation = jnp.where(column == wanted, 1.0, 0.0).astype(BF16)
    for block in range(source.shape[0] // (BLOCK * chunk)):
        moved = mm(permutation, source[block * BLOCK * chunk : (block + 1) * BLOCK * chunk, :])
        moved = moved.astype(BF16)
        at = slice(offset + block * out_rows, offset + (block + 1) * out_rows)
        for h in range(HALVES):
            columns = slice(h * half, (h + 1) * half)
            first = 2 * h * out_rows
            rows[at, columns] = moved[first : first + out_rows]
            scaled[at, columns] = moved[first + out_rows : first + 2 * out_rows]


def hidden_terms(gate_pre, up_pre, hidden_grad):
    gate_pre = gate_pre.astype(BF16).astype(F32)
    up_pre = up_pre.astype(BF16).astype(F32)
    sigmoid = jax.nn.sigmoid(gate_pre)
    activated = gate_pre * sigmoid
    hidden = activated * up_pre
    gate_grad = (hidden_grad * up_pre * sigmoid * (1.0 + gate_pre * (1.0 - sigmoid))).astype(BF16)
    up_grad = (hidden_grad * activated).astype(BF16)
    return hidden, gate_grad, up_grad


def input_kernel(local_experts, quarter, landed, *refs):
    gates, ups, downs = refs[0:4], refs[4:8], refs[8:11]
    down_even, down_odd, out, rows, scaled, coded = refs[11:]
    own, _ = rows.shape
    slots = local_experts * quarter
    devices = own // quarter
    stride = (slots + 1) * SUBLANES
    for i in range(slots, SUBLANES):
        at = slots * SUBLANES + i
        coded[pl.ds(at, devices, stride=stride), :] = jnp.zeros((devices, LANES), F32)
    for expert in range(local_experts):
        land(landed, expert, local_experts, quarter, rows, scaled, 0)
        gate = jnp.concatenate([g[expert] for g in gates], axis=1)
        up = jnp.concatenate([u[expert] for u in ups], axis=1)
        last = (down_even, down_odd)[expert][0]
        down = jnp.concatenate([d[expert] for d in downs] + [last], axis=0)
        hidden_grad = mm(scaled[...], down, NT)
        hidden, gate_grad, up_grad = hidden_terms(mm(rows[...], gate), mm(rows[...], up), hidden_grad)
        product = jnp.sum(hidden_grad * hidden, axis=1, keepdims=True)
        grad = mm(gate_grad, gate, NT) + mm(up_grad, up, NT)
        grad, power, steps = code_rows(grad)
        lane = iota((own, LANES), 1)
        tail = jnp.zeros((own, LANES), F32)
        for at, column in enumerate((power, steps) + code_values(product)):
            tail = jnp.where(lane == at, column, tail)
        for block in range(devices // BLOCK):
            for q in range(quarter):
                at = (block * quarter + q) * BLOCK
                to = block * BLOCK * stride
                slot = expert * quarter + q
                for i in range(SUBLANES):
                    piece = grad[at : at + BLOCK, i * LANES : (i + 1) * LANES]
                    coded[pl.ds(to + slot * SUBLANES + i, BLOCK, stride=stride), :] = piece
                to += slots * SUBLANES + slot
                coded[pl.ds(to, BLOCK, stride=stride), :] = tail[at : at + BLOCK]
    out[...] = to_code(coded[...])


def weight_kernel(local_experts, quarter, source_count, earlier_count, *refs):
    sources, refs = refs[:source_count], refs[source_count:]
    (gate, up, down), refs = refs[:3], refs[3:]
    earlier, refs = refs[:earlier_count], refs[earlier_count:]
    outs, (rows, scaled) = refs[:3], refs[3:]
    chunk = HALVES * 2 * local_experts * quarter
    hidden_width = gate.shape[2]

    def one(expert, carry):
        offset = 0
        for source in sources:
            land(source, expert, local_experts, quarter, rows, scaled, offset)
            offset += source.shape[0] // chunk * quarter
        both = mm(rows[...], jnp.concatenate([gate[expert], up[expert]], axis=1))
        hidden_grad = mm(scaled[...], down[expert], NT)
        hidden, gate_grad, up_grad = hidden_terms(
            both[:, :hidden_width], both[:, hidden_width:], hidden_grad
        )
        grads = mm(rows[...], jnp.concatenate([gate_grad, up_grad], axis=1), TN)
        down_grad = mm(hidden.astype(BF16), scaled[...], TN)
        for at, part in enumerate((grads[:, :hidden_width], grads[:, hidden_width:], down_grad)):
            outs[at][expert] = earlier[at][expert] + part if earlier else part
        return carry

    lax.fori_loop(0, local_experts, one, 0)


def member_rows(member, distance, members, count):
    return pl.ds(pl.multiple_of(lax.rem(member + distance, members) * count, count), count)


def combine_kernel(members, devices, member, coded, pick, *refs):
    outs, total, back = refs[:-2], refs[-2], refs[-1]
    back[...] = from_code(coded[...])
    token_count, tail_width = total.shape
    width = tail_width - LANES
    slots = pick.shape[1] // devices
    stride = (slots + 1) * SUBLANES
    tails = [
        back[pl.ds(slots * SUBLANES + slot, devices, stride=stride), :] for slot in range(slots)
    ]
    tail = jnp.concatenate(tails, axis=0)
    scale = row_scale(tail[:, 0:1], tail[:, 1:2])
    columns = []
    for i in range(SUBLANES):
        pieces = [
            back[pl.ds(slot * SUBLANES + i, devices, stride=stride), :] for slot in range(slots)
        ]
        columns.append(jnp.concatenate(pieces, axis=0))
    grad = jnp.concatenate(columns, axis=1) * scale
    both = pick[0] + pick[1]
    grad, power, steps = code_rows(sum(mm(both, part, TN) for part in split3(grad)))
    total[:, 0:width] = grad
    lane = iota((token_count, LANES), 1)
    total[:, width:] = jnp.where(lane == 0, power, jnp.where(lane == 1, steps, 0.0))
    product = decode_values(tail[:, 2:3], tail[:, 3:4], tail[:, 4:5])
    sums = [jnp.sum(pick[k].astype(F32) * product, axis=0, keepdims=True) for k in range(2)]
    power, coarse, fine = code_values(jnp.concatenate(sums, axis=1))
    spare = jnp.zeros((1, tail_width - 4 * token_count), F32)
    first = jnp.concatenate([power, coarse, spare], axis=1)
    second = jnp.concatenate([fine, jnp.zeros_like(fine), spare], axis=1)
    line = iota((SUBLANES, tail_width), 0)
    lines = to_code(jnp.where(line == 0, first, jnp.where(line == 1, second, 0.0)))
    count = token_count // members
    for out, distance in zip(outs, (0, 1, 3, 2)):
        out[0:count, :] = to_code(total[member_rows(member[0], distance, members, count), :])
        out[count : count + SUBLANES, :] = lines


def sum_kernel(own, from_left, from_right, from_opposite, weights, grad_out, gates_out):
    count, width = grad_out.shape
    token_count = weights.shape[1]
    parts = [from_code(part[...]) for part in (own, from_left, from_right, from_opposite)]
    grads = [
        part[:count, :width] * row_scale(part[:count, width : width + 1], part[:count, width + 1 : width + 2])
        for part in parts
    ]
    grad_out[...] = ((grads[0] + grads[3]) + (grads[1] + grads[2])).astype(BF16)
    values = 2 * token_count
    products = [
        decode_values(
            part[count : count + 1, 0:values],
            part[count : count + 1, values : 2 * values],
            part[count + 1 : count + 2, 0:values],
        )
        for part in parts
    ]
    product = (products[0] + products[3]) + (products[1] + products[2])
    for k in range(2):
        gates_out[k : k + 1, :] = product[:, k * token_count : (k + 1) * token_count] / weights[k : k + 1, :]


def place_kernel(members, member, own, from_left, from_right, from_opposite, out):
    count = own.shape[0]
    for piece, distance in ((own, 0), (from_left, 3), (from_right, 1), (from_opposite, 2)):
        out[member_rows(member[0], distance, members, count), :] = piece[...]


def step(tokens, cotangent, routing, gate_weights, gate_proj, up_proj, down_proj):
    token_count, model_width = tokens.shape
    top_count = routing.shape[1]
    local_experts, _, hidden_width = gate_proj.shape
    groups = lax.axis_size("ep")
    members = lax.axis_size("tp")
    experts = local_experts * groups
    capacity = members * (
        (3 * token_count * top_count + experts * members - 1) // (experts * members)
    )
    quarter = capacity // members
    slots = experts * quarter
    own = groups * quarter
    chunk = HALVES * 2 * local_experts * quarter
    half = model_width // HALVES
    member = lax.axis_index("tp").astype(I32).reshape(1)
    right = [(i, (i + 1) % members) for i in range(members)]
    left = [(i, (i - 1) % members) for i in range(members)]
    across = [(i, (i + 2) % members) for i in range(members)]
    whole = pl.BlockSpec(memory_space=VMEM)
    scalar = pl.BlockSpec(memory_space=SMEM)

    def call(kernel, out_shape, args, scalars=0, scratch=()):
        return pl.pallas_call(
            kernel,
            out_shape=out_shape,
            in_specs=[scalar] * scalars + [whole] * (len(args) - scalars),
            out_specs=jax.tree.map(lambda _: whole, out_shape),
            scratch_shapes=list(scratch),
        )(*args)

    def shape(dims, dtype):
        return jax.ShapeDtypeStruct(dims, dtype)

    gates, ups, downs = [gate_proj], [up_proj], [down_proj]
    for kept, mine in ((gates, gate_proj), (ups, up_proj), (downs, down_proj)):
        kept.append(lax.ppermute(mine, "tp", right))
        kept.append(lax.ppermute(mine, "tp", left))
    gates.append(lax.ppermute(gates[2], "tp", left))
    ups.append(lax.ppermute(ups[1], "tp", right))
    down_even = lax.ppermute(downs[2][0:1], "tp", left)
    down_odd = lax.ppermute(downs[1][1:2], "tp", right)

    send, pick = call(
        lambda *refs: dispatch_kernel(experts, local_experts, quarter, *refs),
        (shape((groups * chunk, half), BF16), shape((2, slots, token_count), BF16)),
        (member, routing.T, gate_weights.T, tokens, cotangent),
        scalars=1,
    )
    landed = lax.all_to_all(
        send.reshape(groups, chunk, half), "ep", split_axis=0, concat_axis=0, tiled=True
    ).reshape(groups * chunk, half)

    middle = groups * chunk // 2
    low, high = landed[:middle], landed[middle:]
    right_low = lax.ppermute(low, "tp", left)
    left_high = lax.ppermute(high, "tp", right)
    right_high = lax.ppermute(high, "tp", left)
    left_low = lax.ppermute(low, "tp", right)
    opposite_low = lax.ppermute(right_low, "tp", left)
    opposite_high = lax.ppermute(left_high, "tp", right)

    back_rows = (local_experts * quarter + 1) * SUBLANES
    back = call(
        lambda *refs: input_kernel(local_experts, quarter, *refs),
        shape((groups * back_rows, LANES), I16),
        (landed, *gates, *ups, *downs, down_even, down_odd),
        scratch=[VMEM((own, model_width), BF16)] * 2 + [VMEM((groups * back_rows, LANES), F32)],
    )
    back = back.reshape(groups, back_rows, LANES)
    back = lax.all_to_all(back, "ep", split_axis=0, concat_axis=0, tiled=True)
    back = back.reshape(groups * back_rows, LANES)
    count = token_count // members
    tail_width = model_width + LANES
    part = shape((count + SUBLANES, tail_width), I16)
    mine, to_right, to_left, to_across = call(
        lambda *refs: combine_kernel(members, groups, *refs),
        (part,) * 4,
        (member, back, pick),
        scalars=1,
        scratch=[VMEM((token_count, tail_width), F32), VMEM((groups * back_rows, LANES), F32)],
    )
    pieces = (
        lax.ppermute(to_right, "tp", right),
        lax.ppermute(to_left, "tp", left),
        lax.ppermute(to_across, "tp", across),
    )
    summed, gates_grad = call(
        sum_kernel,
        (shape((count, model_width), BF16), shape((top_count, token_count), F32)),
        (mine, *pieces, gate_weights.T),
    )
    pieces = (
        lax.ppermute(summed, "tp", right),
        lax.ppermute(summed, "tp", left),
        lax.ppermute(summed, "tp", across),
    )
    tokens_grad = call(
        lambda *refs: place_kernel(members, *refs),
        shape((token_count, model_width), BF16),
        (member, summed, *pieces),
        scalars=1,
    )

    sums = (
        shape((local_experts, model_width, hidden_width), F32),
        shape((local_experts, model_width, hidden_width), F32),
        shape((local_experts, hidden_width, model_width), F32),
    )

    def weight_sums(sources, earlier):
        count = sum(source.shape[0] for source in sources) // chunk * quarter
        return call(
            lambda *refs: weight_kernel(local_experts, quarter, len(sources), len(earlier), *refs),
            sums,
            (*sources, gate_proj, up_proj, down_proj, *earlier),
            scratch=[VMEM((count, model_width), BF16)] * 2,
        )

    near = weight_sums((landed, left_low, left_high, right_low, right_high), ())
    gate_grad, up_grad, down_grad = weight_sums((opposite_low, opposite_high), near)
    return (tokens_grad, gates_grad.T, gate_grad, up_grad, down_grad)


def solution(mesh):
    in_specs = (
        P("ep", None),
        P("ep", None),
        P("ep", None),
        P("ep", None),
        P("ep", None, "tp"),
        P("ep", None, "tp"),
        P("ep", "tp", None),
    )
    out_specs = (
        P("ep", None),
        P("ep", None),
        P("ep", None, "tp"),
        P("ep", None, "tp"),
        P("ep", "tp", None),
    )
    return jax.shard_map(step, mesh=mesh, in_specs=in_specs, out_specs=out_specs, check_vma=False)
```

```python
import jax
import jax.numpy as jnp
from jax import lax
from jax.experimental import pallas as pl
from jax.experimental.pallas import tpu as pltpu
from jax.sharding import PartitionSpec as P


F32 = jnp.float32
I16 = jnp.int16
BF16 = jnp.bfloat16
I32 = jnp.int32
LANES = 128
SUBLANES = 8
BLOCK = 16
HALVES = 2
TOP_CODE = 32766.0
STEPS = 8192.0
FINE = 32768.0
VMEM = pltpu.VMEM
SMEM = pltpu.SMEM
NN = ((1,), (0,))
NT = ((1,), (1,))
TN = ((0,), (0,))


def mm(a, b, dims=NN):
    return lax.dot_general(a, b, (dims, ((), ())), preferred_element_type=F32)


def iota(shape, dim):
    return lax.broadcasted_iota(I32, shape, dim)


def split3(value):
    high = value.astype(BF16)
    rest = value - high.astype(F32)
    middle = rest.astype(BF16)
    low = (rest - middle.astype(F32)).astype(BF16)
    return high, middle, low


def exponent(value):
    return jnp.floor(jnp.log(jnp.maximum(value, 1e-30)) * 1.4426950408889634)


def row_scale(power, steps):
    return steps * jnp.exp2(power) * (1.0 / (STEPS * TOP_CODE))


def code_rows(value):
    largest = jnp.maximum(jnp.max(jnp.abs(value), axis=1, keepdims=True), 1e-30)
    power = exponent(largest)
    steps = jnp.ceil(largest * jnp.exp2(-power) * STEPS)
    return jnp.round(value * (1.0 / row_scale(power, steps))), power, steps


def code_values(value):
    power = exponent(jnp.abs(value))
    value = value * jnp.exp2(-power) * STEPS
    coarse = jnp.round(value)
    return power, coarse, jnp.round((value - coarse) * FINE)


def decode_values(power, coarse, fine):
    return (coarse + fine * (1.0 / FINE)) * (jnp.exp2(power) * (1.0 / STEPS))


def to_code(value):
    return value.astype(I32).astype(I16)


def from_code(value):
    return value.astype(I32).astype(F32)


def dispatch_kernel(
    experts, local_experts, quarter, member, routing, weights, tokens, cotangent, rows_out, pick
):
    token_count, width = tokens.shape
    half = width // HALVES
    row_count = rows_out.shape[0]
    slots = pick.shape[1]
    group = local_experts * quarter
    chunk = HALVES * 2 * group
    devices = experts // local_experts
    expert = iota((experts, token_count), 0)
    chosen = [routing[k : k + 1, :] for k in range(2)]
    onehot = [jnp.where(expert == c, 1.0, 0.0) for c in chosen]
    earlier = iota((token_count, token_count), 0)
    later = iota((token_count, token_count), 1)
    upper = jnp.where(earlier < later, 1.0, 0.0).astype(BF16)
    before = mm((onehot[0] + onehot[1]).astype(BF16), upper)
    row = iota((row_count, token_count), 0)
    slot = iota((slots, token_count), 0)
    token_rows = []
    for k in range(2):
        position = jnp.sum(onehot[k] * before, axis=0, keepdims=True).astype(I32)
        local = position - member[0] * quarter
        present = (local >= 0) & (local < quarter)
        device = chosen[k] // local_experts
        within = (chosen[k] - device * local_experts) * quarter + local
        pick[k] = jnp.where(slot == jnp.where(present, within * devices + device, -1), 1.0, 0.0).astype(BF16)
        token_rows.append(jnp.where(present, device * chunk + within, -chunk))
    total = None
    for h in range(HALVES):
        columns = slice(h * half, (h + 1) * half)
        base = h * 2 * group
        hits = [row == r + base for r in token_rows]
        part = mm(jnp.where(hits[0] | hits[1], 1.0, 0.0).astype(BF16), tokens[:, columns])
        hits = [row == r + (base + group) for r in token_rows]
        weighted = jnp.where(hits[0], weights[0:1, :], jnp.where(hits[1], weights[1:2, :], 0.0))
        slot_weight = jnp.sum(weighted, axis=1, keepdims=True)
        chosen_rows = jnp.where(hits[0] | hits[1], 1.0, 0.0).astype(BF16)
        part = part + slot_weight * mm(chosen_rows, cotangent[:, columns])
        total = part if total is None else total + part
    rows_out[...] = total.astype(BF16)


def land(source, expert, local_experts, quarter, rows, scaled, offset):
    half = source.shape[1]
    group = local_experts * quarter
    chunk = HALVES * 2 * group
    out_rows = BLOCK * quarter
    index = iota((HALVES * 2 * out_rows, 1), 0)
    kind = index // out_rows
    rest = index - kind * out_rows
    slot = rest // BLOCK
    wanted = (rest - slot * BLOCK) * chunk + kind * group + expert * quarter + slot
    column = iota((HALVES * 2 * out_rows, BLOCK * chunk), 1)
    permutation = jnp.where(column == wanted, 1.0, 0.0).astype(BF16)
    for block in range(source.shape[0] // (BLOCK * chunk)):
        moved = mm(permutation, source[block * BLOCK * chunk : (block + 1) * BLOCK * chunk, :])
        moved = moved.astype(BF16)
        at = slice(offset + block * out_rows, offset + (block + 1) * out_rows)
        for h in range(HALVES):
            columns = slice(h * half, (h + 1) * half)
            first = 2 * h * out_rows
            rows[at, columns] = moved[first : first + out_rows]
            scaled[at, columns] = moved[first + out_rows : first + 2 * out_rows]


def hidden_terms(gate_pre, up_pre, hidden_grad):
    gate_pre = gate_pre.astype(BF16).astype(F32)
    up_pre = up_pre.astype(BF16).astype(F32)
    sigmoid = jax.nn.sigmoid(gate_pre)
    activated = gate_pre * sigmoid
    hidden = activated * up_pre
    gate_grad = (hidden_grad * up_pre * sigmoid * (1.0 + gate_pre * (1.0 - sigmoid))).astype(BF16)
    up_grad = (hidden_grad * activated).astype(BF16)
    return hidden, gate_grad, up_grad


def input_kernel(local_experts, quarter, landed, *refs):
    gates, ups, downs = refs[0:4], refs[4:8], refs[8:11]
    down_even, down_odd, out, rows, scaled, coded = refs[11:]
    own, _ = rows.shape
    slots = local_experts * quarter
    devices = own // quarter
    stride = (slots + 1) * SUBLANES
    for i in range(slots, SUBLANES):
        at = slots * SUBLANES + i
        coded[pl.ds(at, devices, stride=stride), :] = jnp.zeros((devices, LANES), F32)
    for expert in range(local_experts):
        land(landed, expert, local_experts, quarter, rows, scaled, 0)
        gate = jnp.concatenate([g[expert] for g in gates], axis=1)
        up = jnp.concatenate([u[expert] for u in ups], axis=1)
        last = (down_even, down_odd)[expert][0]
        down = jnp.concatenate([d[expert] for d in downs] + [last], axis=0)
        hidden_grad = mm(scaled[...], down, NT)
        hidden, gate_grad, up_grad = hidden_terms(mm(rows[...], gate), mm(rows[...], up), hidden_grad)
        product = jnp.sum(hidden_grad * hidden, axis=1, keepdims=True)
        grad = mm(gate_grad, gate, NT) + mm(up_grad, up, NT)
        grad, power, steps = code_rows(grad)
        lane = iota((own, LANES), 1)
        tail = jnp.zeros((own, LANES), F32)
        for at, column in enumerate((power, steps) + code_values(product)):
            tail = jnp.where(lane == at, column, tail)
        for block in range(devices // BLOCK):
            for q in range(quarter):
                at = (block * quarter + q) * BLOCK
                to = block * BLOCK * stride
                slot = expert * quarter + q
                for i in range(SUBLANES):
                    piece = grad[at : at + BLOCK, i * LANES : (i + 1) * LANES]
                    coded[pl.ds(to + slot * SUBLANES + i, BLOCK, stride=stride), :] = piece
                to += slots * SUBLANES + slot
                coded[pl.ds(to, BLOCK, stride=stride), :] = tail[at : at + BLOCK]
    out[...] = to_code(coded[...])


def weight_kernel(local_experts, quarter, source_count, earlier_count, *refs):
    sources, refs = refs[:source_count], refs[source_count:]
    (gate, up, down), refs = refs[:3], refs[3:]
    earlier, refs = refs[:earlier_count], refs[earlier_count:]
    outs, (rows, scaled) = refs[:3], refs[3:]
    chunk = HALVES * 2 * local_experts * quarter
    hidden_width = gate.shape[2]

    def one(expert, carry):
        offset = 0
        for source in sources:
            land(source, expert, local_experts, quarter, rows, scaled, offset)
            offset += source.shape[0] // chunk * quarter
        both = mm(rows[...], jnp.concatenate([gate[expert], up[expert]], axis=1))
        hidden_grad = mm(scaled[...], down[expert], NT)
        hidden, gate_grad, up_grad = hidden_terms(
            both[:, :hidden_width], both[:, hidden_width:], hidden_grad
        )
        grads = mm(rows[...], jnp.concatenate([gate_grad, up_grad], axis=1), TN)
        down_grad = mm(hidden.astype(BF16), scaled[...], TN)
        for at, part in enumerate((grads[:, :hidden_width], grads[:, hidden_width:], down_grad)):
            outs[at][expert] = earlier[at][expert] + part if earlier else part
        return carry

    lax.fori_loop(0, local_experts, one, 0)


def member_rows(member, distance, members, count):
    return pl.ds(pl.multiple_of(lax.rem(member + distance, members) * count, count), count)


def combine_kernel(members, devices, member, coded, pick, *refs):
    outs, total, back = refs[:-2], refs[-2], refs[-1]
    back[...] = from_code(coded[...])
    token_count, tail_width = total.shape
    width = tail_width - LANES
    slots = pick.shape[1] // devices
    stride = (slots + 1) * SUBLANES
    tails = [
        back[pl.ds(slots * SUBLANES + slot, devices, stride=stride), :] for slot in range(slots)
    ]
    tail = jnp.concatenate(tails, axis=0)
    scale = row_scale(tail[:, 0:1], tail[:, 1:2])
    columns = []
    for i in range(SUBLANES):
        pieces = [
            back[pl.ds(slot * SUBLANES + i, devices, stride=stride), :] for slot in range(slots)
        ]
        columns.append(jnp.concatenate(pieces, axis=0))
    grad = jnp.concatenate(columns, axis=1) * scale
    both = pick[0] + pick[1]
    grad, power, steps = code_rows(sum(mm(both, part, TN) for part in split3(grad)))
    total[:, 0:width] = grad
    lane = iota((token_count, LANES), 1)
    total[:, width:] = jnp.where(lane == 0, power, jnp.where(lane == 1, steps, 0.0))
    product = decode_values(tail[:, 2:3], tail[:, 3:4], tail[:, 4:5])
    sums = [jnp.sum(pick[k].astype(F32) * product, axis=0, keepdims=True) for k in range(2)]
    power, coarse, fine = code_values(jnp.concatenate(sums, axis=1))
    spare = jnp.zeros((1, tail_width - 4 * token_count), F32)
    first = jnp.concatenate([power, coarse, spare], axis=1)
    second = jnp.concatenate([fine, jnp.zeros_like(fine), spare], axis=1)
    line = iota((SUBLANES, tail_width), 0)
    lines = to_code(jnp.where(line == 0, first, jnp.where(line == 1, second, 0.0)))
    count = token_count // members
    for out, distance in zip(outs, (0, 1, 3, 2)):
        out[0:count, :] = to_code(total[member_rows(member[0], distance, members, count), :])
        out[count : count + SUBLANES, :] = lines


def sum_kernel(own, from_left, from_right, from_opposite, weights, grad_out, gates_out):
    count, width = grad_out.shape
    token_count = weights.shape[1]
    parts = [from_code(part[...]) for part in (own, from_left, from_right, from_opposite)]
    grads = [
        part[:count, :width] * row_scale(part[:count, width : width + 1], part[:count, width + 1 : width + 2])
        for part in parts
    ]
    grad_out[...] = ((grads[0] + grads[3]) + (grads[1] + grads[2])).astype(BF16)
    values = 2 * token_count
    products = [
        decode_values(
            part[count : count + 1, 0:values],
            part[count : count + 1, values : 2 * values],
            part[count + 1 : count + 2, 0:values],
        )
        for part in parts
    ]
    product = (products[0] + products[3]) + (products[1] + products[2])
    for k in range(2):
        gates_out[k : k + 1, :] = product[:, k * token_count : (k + 1) * token_count] / weights[k : k + 1, :]


def place_kernel(members, member, own, from_left, from_right, from_opposite, out):
    count = own.shape[0]
    for piece, distance in ((own, 0), (from_left, 3), (from_right, 1), (from_opposite, 2)):
        out[member_rows(member[0], distance, members, count), :] = piece[...]


def step(tokens, cotangent, routing, gate_weights, gate_proj, up_proj, down_proj):
    token_count, model_width = tokens.shape
    top_count = routing.shape[1]
    local_experts, _, hidden_width = gate_proj.shape
    groups = lax.axis_size("ep")
    members = lax.axis_size("tp")
    experts = local_experts * groups
    capacity = members * (
        (3 * token_count * top_count + experts * members - 1) // (experts * members)
    )
    quarter = capacity // members
    slots = experts * quarter
    own = groups * quarter
    chunk = HALVES * 2 * local_experts * quarter
    half = model_width // HALVES
    member = lax.axis_index("tp").astype(I32).reshape(1)
    right = [(i, (i + 1) % members) for i in range(members)]
    left = [(i, (i - 1) % members) for i in range(members)]
    across = [(i, (i + 2) % members) for i in range(members)]
    whole = pl.BlockSpec(memory_space=VMEM)
    scalar = pl.BlockSpec(memory_space=SMEM)

    def call(kernel, out_shape, args, scalars=0, scratch=()):
        return pl.pallas_call(
            kernel,
            out_shape=out_shape,
            in_specs=[scalar] * scalars + [whole] * (len(args) - scalars),
            out_specs=jax.tree.map(lambda _: whole, out_shape),
            scratch_shapes=list(scratch),
        )(*args)

    def shape(dims, dtype):
        return jax.ShapeDtypeStruct(dims, dtype)

    gates, ups, downs = [gate_proj], [up_proj], [down_proj]
    for kept, mine in ((gates, gate_proj), (ups, up_proj), (downs, down_proj)):
        kept.append(lax.ppermute(mine, "tp", right))
        kept.append(lax.ppermute(mine, "tp", left))
    gates.append(lax.ppermute(gates[2], "tp", left))
    ups.append(lax.ppermute(ups[1], "tp", right))
    down_even = lax.ppermute(downs[2][0:1], "tp", left)
    down_odd = lax.ppermute(downs[1][1:2], "tp", right)

    send, pick = call(
        lambda *refs: dispatch_kernel(experts, local_experts, quarter, *refs),
        (shape((groups * chunk, half), BF16), shape((2, slots, token_count), BF16)),
        (member, routing.T, gate_weights.T, tokens, cotangent),
        scalars=1,
    )
    landed = lax.all_to_all(
        send.reshape(groups, chunk, half), "ep", split_axis=0, concat_axis=0, tiled=True
    ).reshape(groups * chunk, half)

    middle = groups * chunk // 2
    low, high = landed[:middle], landed[middle:]
    right_low = lax.ppermute(low, "tp", left)
    left_high = lax.ppermute(high, "tp", right)
    right_high = lax.ppermute(high, "tp", left)
    left_low = lax.ppermute(low, "tp", right)
    opposite_low = lax.ppermute(right_low, "tp", left)
    opposite_high = lax.ppermute(left_high, "tp", right)

    back_rows = (local_experts * quarter + 1) * SUBLANES
    back = call(
        lambda *refs: input_kernel(local_experts, quarter, *refs),
        shape((groups * back_rows, LANES), I16),
        (landed, *gates, *ups, *downs, down_even, down_odd),
        scratch=[VMEM((own, model_width), BF16)] * 2 + [VMEM((groups * back_rows, LANES), F32)],
    )
    back = back.reshape(groups, back_rows, LANES)
    back = lax.all_to_all(back, "ep", split_axis=0, concat_axis=0, tiled=True)
    back = back.reshape(groups * back_rows, LANES)
    count = token_count // members
    tail_width = model_width + LANES
    part = shape((count + SUBLANES, tail_width), I16)
    mine, to_right, to_left, to_across = call(
        lambda *refs: combine_kernel(members, groups, *refs),
        (part,) * 4,
        (member, back, pick),
        scalars=1,
        scratch=[VMEM((token_count, tail_width), F32), VMEM((groups * back_rows, LANES), F32)],
    )
    pieces = (
        lax.ppermute(to_right, "tp", right),
        lax.ppermute(to_left, "tp", left),
        lax.ppermute(to_across, "tp", across),
    )
    summed, gates_grad = call(
        sum_kernel,
        (shape((count, model_width), BF16), shape((top_count, token_count), F32)),
        (mine, *pieces, gate_weights.T),
    )
    pieces = (
        lax.ppermute(summed, "tp", right),
        lax.ppermute(summed, "tp", left),
        lax.ppermute(summed, "tp", across),
    )
    tokens_grad = call(
        lambda *refs: place_kernel(members, *refs),
        shape((token_count, model_width), BF16),
        (member, summed, *pieces),
        scalars=1,
    )

    sums = (
        shape((local_experts, model_width, hidden_width), F32),
        shape((local_experts, model_width, hidden_width), F32),
        shape((local_experts, hidden_width, model_width), F32),
    )

    def weight_sums(sources, earlier):
        count = sum(source.shape[0] for source in sources) // chunk * quarter
        return call(
            lambda *refs: weight_kernel(local_experts, quarter, len(sources), len(earlier), *refs),
            sums,
            (*sources, gate_proj, up_proj, down_proj, *earlier),
            scratch=[VMEM((count, model_width), BF16)] * 2,
        )

    near = weight_sums((landed, right_low, left_high), ())
    far = (right_high, left_low, opposite_low, opposite_high)
    gate_grad, up_grad, down_grad = weight_sums(far, near)
    return (tokens_grad, gates_grad.T, gate_grad, up_grad, down_grad)


def solution(mesh):
    in_specs = (
        P("ep", None),
        P("ep", None),
        P("ep", None),
        P("ep", None),
        P("ep", None, "tp"),
        P("ep", None, "tp"),
        P("ep", "tp", None),
    )
    out_specs = (
        P("ep", None),
        P("ep", None),
        P("ep", None, "tp"),
        P("ep", None, "tp"),
        P("ep", "tp", None),
    )
    return jax.shard_map(step, mesh=mesh, in_specs=in_specs, out_specs=out_specs, check_vma=False)
```

```python
import jax
import jax.numpy as jnp
from jax import lax
from jax.experimental import pallas as pl
from jax.experimental.pallas import tpu as pltpu
from jax.sharding import PartitionSpec as P


F32 = jnp.float32
I16 = jnp.int16
BF16 = jnp.bfloat16
I32 = jnp.int32
LANES = 128
SUBLANES = 8
BLOCK = 16
HALVES = 2
TOP_CODE = 32766.0
STEPS = 8192.0
FINE = 32768.0
VMEM = pltpu.VMEM
SMEM = pltpu.SMEM
NN = ((1,), (0,))
NT = ((1,), (1,))
TN = ((0,), (0,))


def mm(a, b, dims=NN):
    return lax.dot_general(a, b, (dims, ((), ())), preferred_element_type=F32)


def iota(shape, dim):
    return lax.broadcasted_iota(I32, shape, dim)


def split3(value):
    high = value.astype(BF16)
    rest = value - high.astype(F32)
    middle = rest.astype(BF16)
    low = (rest - middle.astype(F32)).astype(BF16)
    return high, middle, low


def exponent(value):
    return jnp.floor(jnp.log(jnp.maximum(value, 1e-30)) * 1.4426950408889634)


def row_scale(power, steps):
    return steps * jnp.exp2(power) * (1.0 / (STEPS * TOP_CODE))


def code_rows(value):
    largest = jnp.maximum(jnp.max(jnp.abs(value), axis=1, keepdims=True), 1e-30)
    power = exponent(largest)
    steps = jnp.ceil(largest * jnp.exp2(-power) * STEPS)
    return jnp.round(value * (1.0 / row_scale(power, steps))), power, steps


def code_values(value):
    power = exponent(jnp.abs(value))
    value = value * jnp.exp2(-power) * STEPS
    coarse = jnp.round(value)
    return power, coarse, jnp.round((value - coarse) * FINE)


def decode_values(power, coarse, fine):
    return (coarse + fine * (1.0 / FINE)) * (jnp.exp2(power) * (1.0 / STEPS))


def to_code(value):
    return value.astype(I32).astype(I16)


def from_code(value):
    return value.astype(I32).astype(F32)


def dispatch_kernel(
    experts, local_experts, quarter, member, routing, weights, tokens, cotangent, rows_out, pick, laid
):
    token_count, _ = tokens.shape
    slots = pick.shape[1]
    group = local_experts * quarter
    devices = experts // local_experts
    expert = iota((experts, token_count), 0)
    chosen = [routing[k : k + 1, :] for k in range(2)]
    onehot = [jnp.where(expert == c, 1.0, 0.0) for c in chosen]
    earlier = iota((token_count, token_count), 0)
    later = iota((token_count, token_count), 1)
    upper = jnp.where(earlier < later, 1.0, 0.0).astype(BF16)
    before = mm((onehot[0] + onehot[1]).astype(BF16), upper)
    slot = iota((slots, token_count), 0)
    hits = []
    for k in range(2):
        position = jnp.sum(onehot[k] * before, axis=0, keepdims=True).astype(I32)
        local = position - member[0] * quarter
        present = (local >= 0) & (local < quarter)
        device = chosen[k] // local_experts
        within = (chosen[k] - device * local_experts) * quarter + local
        hits.append(slot == jnp.where(present, within * devices + device, -1))
        pick[k] = jnp.where(hits[k], 1.0, 0.0).astype(BF16)
    weighted = jnp.where(hits[0], weights[0:1, :], jnp.where(hits[1], weights[1:2, :], 0.0))
    slot_weight = jnp.sum(weighted, axis=1, keepdims=True)
    both = jnp.where(hits[0] | hits[1], 1.0, 0.0).astype(BF16)
    values = (mm(both, tokens[...]), mm(both, cotangent[...]) * slot_weight)
    tiles = laid.shape[0]
    chunk = HALVES * 2 * group
    for kind, value in enumerate(values):
        for h in range(HALVES):
            for at in range(group):
                to = (2 * h + kind) * group + at
                for tile in range(tiles):
                    column = (h * tiles + tile) * LANES
                    piece = value[at * devices : (at + 1) * devices, column : column + LANES]
                    laid[tile, pl.ds(to, devices, stride=chunk), :] = piece
    for tile in range(tiles):
        rows_out[:, tile * LANES : (tile + 1) * LANES] = laid[tile].astype(BF16)


def land(source, expert, local_experts, quarter, rows, scaled, offset):
    half = source.shape[1]
    group = local_experts * quarter
    chunk = HALVES * 2 * group
    out_rows = BLOCK * quarter
    index = iota((HALVES * 2 * out_rows, 1), 0)
    kind = index // out_rows
    rest = index - kind * out_rows
    slot = rest // BLOCK
    wanted = (rest - slot * BLOCK) * chunk + kind * group + expert * quarter + slot
    column = iota((HALVES * 2 * out_rows, BLOCK * chunk), 1)
    permutation = jnp.where(column == wanted, 1.0, 0.0).astype(BF16)
    for block in range(source.shape[0] // (BLOCK * chunk)):
        moved = mm(permutation, source[block * BLOCK * chunk : (block + 1) * BLOCK * chunk, :])
        moved = moved.astype(BF16)
        at = slice(offset + block * out_rows, offset + (block + 1) * out_rows)
        for h in range(HALVES):
            columns = slice(h * half, (h + 1) * half)
            first = 2 * h * out_rows
            rows[at, columns] = moved[first : first + out_rows]
            scaled[at, columns] = moved[first + out_rows : first + 2 * out_rows]


def hidden_terms(gate_pre, up_pre, hidden_grad):
    gate_pre = gate_pre.astype(BF16).astype(F32)
    up_pre = up_pre.astype(BF16).astype(F32)
    sigmoid = jax.nn.sigmoid(gate_pre)
    activated = gate_pre * sigmoid
    hidden = activated * up_pre
    gate_grad = (hidden_grad * up_pre * sigmoid * (1.0 + gate_pre * (1.0 - sigmoid))).astype(BF16)
    up_grad = (hidden_grad * activated).astype(BF16)
    return hidden, gate_grad, up_grad


def input_kernel(local_experts, quarter, landed, *refs):
    gates, ups, downs = refs[0:4], refs[4:8], refs[8:11]
    down_even, down_odd, out, rows, scaled, coded = refs[11:]
    own, _ = rows.shape
    slots = local_experts * quarter
    devices = own // quarter
    stride = (slots + 1) * SUBLANES
    for i in range(slots, SUBLANES):
        at = slots * SUBLANES + i
        coded[pl.ds(at, devices, stride=stride), :] = jnp.zeros((devices, LANES), F32)
    for expert in range(local_experts):
        land(landed, expert, local_experts, quarter, rows, scaled, 0)
        gate = jnp.concatenate([g[expert] for g in gates], axis=1)
        up = jnp.concatenate([u[expert] for u in ups], axis=1)
        last = (down_even, down_odd)[expert][0]
        down = jnp.concatenate([d[expert] for d in downs] + [last], axis=0)
        hidden_grad = mm(scaled[...], down, NT)
        hidden, gate_grad, up_grad = hidden_terms(mm(rows[...], gate), mm(rows[...], up), hidden_grad)
        product = jnp.sum(hidden_grad * hidden, axis=1, keepdims=True)
        grad = mm(gate_grad, gate, NT) + mm(up_grad, up, NT)
        grad, power, steps = code_rows(grad)
        lane = iota((own, LANES), 1)
        tail = jnp.zeros((own, LANES), F32)
        for at, column in enumerate((power, steps) + code_values(product)):
            tail = jnp.where(lane == at, column, tail)
        for block in range(devices // BLOCK):
            for q in range(quarter):
                at = (block * quarter + q) * BLOCK
                to = block * BLOCK * stride
                slot = expert * quarter + q
                for i in range(SUBLANES):
                    piece = grad[at : at + BLOCK, i * LANES : (i + 1) * LANES]
                    coded[pl.ds(to + slot * SUBLANES + i, BLOCK, stride=stride), :] = piece
                to += slots * SUBLANES + slot
                coded[pl.ds(to, BLOCK, stride=stride), :] = tail[at : at + BLOCK]
    out[...] = to_code(coded[...])


def weight_kernel(local_experts, quarter, source_count, earlier_count, *refs):
    sources, refs = refs[:source_count], refs[source_count:]
    (gate, up, down), refs = refs[:3], refs[3:]
    earlier, refs = refs[:earlier_count], refs[earlier_count:]
    outs, (rows, scaled) = refs[:3], refs[3:]
    chunk = HALVES * 2 * local_experts * quarter
    hidden_width = gate.shape[2]

    def one(expert, carry):
        offset = 0
        for source in sources:
            land(source, expert, local_experts, quarter, rows, scaled, offset)
            offset += source.shape[0] // chunk * quarter
        both = mm(rows[...], jnp.concatenate([gate[expert], up[expert]], axis=1))
        hidden_grad = mm(scaled[...], down[expert], NT)
        hidden, gate_grad, up_grad = hidden_terms(
            both[:, :hidden_width], both[:, hidden_width:], hidden_grad
        )
        grads = mm(rows[...], jnp.concatenate([gate_grad, up_grad], axis=1), TN)
        down_grad = mm(hidden.astype(BF16), scaled[...], TN)
        for at, part in enumerate((grads[:, :hidden_width], grads[:, hidden_width:], down_grad)):
            outs[at][expert] = earlier[at][expert] + part if earlier else part
        return carry

    lax.fori_loop(0, local_experts, one, 0)


def member_rows(member, distance, members, count):
    return pl.ds(pl.multiple_of(lax.rem(member + distance, members) * count, count), count)


def combine_kernel(members, devices, member, coded, pick, *refs):
    outs, total, back = refs[:-2], refs[-2], refs[-1]
    back[...] = from_code(coded[...])
    token_count, tail_width = total.shape
    width = tail_width - LANES
    slots = pick.shape[1] // devices
    stride = (slots + 1) * SUBLANES
    tails = [
        back[pl.ds(slots * SUBLANES + slot, devices, stride=stride), :] for slot in range(slots)
    ]
    tail = jnp.concatenate(tails, axis=0)
    scale = row_scale(tail[:, 0:1], tail[:, 1:2])
    columns = []
    for i in range(SUBLANES):
        pieces = [
            back[pl.ds(slot * SUBLANES + i, devices, stride=stride), :] for slot in range(slots)
        ]
        columns.append(jnp.concatenate(pieces, axis=0))
    grad = jnp.concatenate(columns, axis=1) * scale
    both = pick[0] + pick[1]
    grad, power, steps = code_rows(sum(mm(both, part, TN) for part in split3(grad)[:2]))
    total[:, 0:width] = grad
    lane = iota((token_count, LANES), 1)
    total[:, width:] = jnp.where(lane == 0, power, jnp.where(lane == 1, steps, 0.0))
    product = decode_values(tail[:, 2:3], tail[:, 3:4], tail[:, 4:5])
    sums = [jnp.sum(pick[k].astype(F32) * product, axis=0, keepdims=True) for k in range(2)]
    power, coarse, fine = code_values(jnp.concatenate(sums, axis=1))
    spare = jnp.zeros((1, tail_width - 4 * token_count), F32)
    first = jnp.concatenate([power, coarse, spare], axis=1)
    second = jnp.concatenate([fine, jnp.zeros_like(fine), spare], axis=1)
    line = iota((SUBLANES, tail_width), 0)
    lines = to_code(jnp.where(line == 0, first, jnp.where(line == 1, second, 0.0)))
    count = token_count // members
    for out, distance in zip(outs, (0, 1, 3, 2)):
        out[0:count, :] = to_code(total[member_rows(member[0], distance, members, count), :])
        out[count : count + SUBLANES, :] = lines


def sum_kernel(own, from_left, from_right, from_opposite, weights, grad_out, gates_out):
    count, width = grad_out.shape
    token_count = weights.shape[1]
    parts = [from_code(part[...]) for part in (own, from_left, from_right, from_opposite)]
    grads = [
        part[:count, :width] * row_scale(part[:count, width : width + 1], part[:count, width + 1 : width + 2])
        for part in parts
    ]
    grad_out[...] = ((grads[0] + grads[3]) + (grads[1] + grads[2])).astype(BF16)
    values = 2 * token_count
    products = [
        decode_values(
            part[count : count + 1, 0:values],
            part[count : count + 1, values : 2 * values],
            part[count + 1 : count + 2, 0:values],
        )
        for part in parts
    ]
    product = (products[0] + products[3]) + (products[1] + products[2])
    for k in range(2):
        gates_out[k : k + 1, :] = product[:, k * token_count : (k + 1) * token_count] / weights[k : k + 1, :]


def place_kernel(members, member, own, from_left, from_right, from_opposite, out):
    count = own.shape[0]
    for piece, distance in ((own, 0), (from_left, 3), (from_right, 1), (from_opposite, 2)):
        out[member_rows(member[0], distance, members, count), :] = piece[...]


def step(tokens, cotangent, routing, gate_weights, gate_proj, up_proj, down_proj):
    token_count, model_width = tokens.shape
    top_count = routing.shape[1]
    local_experts, _, hidden_width = gate_proj.shape
    groups = lax.axis_size("ep")
    members = lax.axis_size("tp")
    experts = local_experts * groups
    capacity = members * (
        (3 * token_count * top_count + experts * members - 1) // (experts * members)
    )
    quarter = capacity // members
    slots = experts * quarter
    own = groups * quarter
    chunk = HALVES * 2 * local_experts * quarter
    half = model_width // HALVES
    member = lax.axis_index("tp").astype(I32).reshape(1)
    right = [(i, (i + 1) % members) for i in range(members)]
    left = [(i, (i - 1) % members) for i in range(members)]
    across = [(i, (i + 2) % members) for i in range(members)]
    whole = pl.BlockSpec(memory_space=VMEM)
    scalar = pl.BlockSpec(memory_space=SMEM)

    def call(kernel, out_shape, args, scalars=0, scratch=()):
        return pl.pallas_call(
            kernel,
            out_shape=out_shape,
            in_specs=[scalar] * scalars + [whole] * (len(args) - scalars),
            out_specs=jax.tree.map(lambda _: whole, out_shape),
            scratch_shapes=list(scratch),
        )(*args)

    def shape(dims, dtype):
        return jax.ShapeDtypeStruct(dims, dtype)

    gates, ups, downs = [gate_proj], [up_proj], [down_proj]
    for kept, mine in ((gates, gate_proj), (ups, up_proj), (downs, down_proj)):
        kept.append(lax.ppermute(mine, "tp", right))
        kept.append(lax.ppermute(mine, "tp", left))
    gates.append(lax.ppermute(gates[2], "tp", left))
    ups.append(lax.ppermute(ups[1], "tp", right))
    down_even = lax.ppermute(downs[2][0:1], "tp", left)
    down_odd = lax.ppermute(downs[1][1:2], "tp", right)

    send, pick = call(
        lambda *refs: dispatch_kernel(experts, local_experts, quarter, *refs),
        (shape((groups * chunk, half), BF16), shape((2, slots, token_count), BF16)),
        (member, routing.T, gate_weights.T, tokens, cotangent),
        scalars=1,
        scratch=[VMEM((half // LANES, groups * chunk, LANES), F32)],
    )
    landed = lax.all_to_all(
        send.reshape(groups, chunk, half), "ep", split_axis=0, concat_axis=0, tiled=True
    ).reshape(groups * chunk, half)

    middle = groups * chunk // 2
    low, high = landed[:middle], landed[middle:]
    right_low = lax.ppermute(low, "tp", left)
    left_high = lax.ppermute(high, "tp", right)
    right_high = lax.ppermute(high, "tp", left)
    left_low = lax.ppermute(low, "tp", right)
    opposite_low = lax.ppermute(right_low, "tp", left)
    opposite_high = lax.ppermute(left_high, "tp", right)

    back_rows = (local_experts * quarter + 1) * SUBLANES
    back = call(
        lambda *refs: input_kernel(local_experts, quarter, *refs),
        shape((groups * back_rows, LANES), I16),
        (landed, *gates, *ups, *downs, down_even, down_odd),
        scratch=[VMEM((own, model_width), BF16)] * 2 + [VMEM((groups * back_rows, LANES), F32)],
    )
    back = back.reshape(groups, back_rows, LANES)
    back = lax.all_to_all(back, "ep", split_axis=0, concat_axis=0, tiled=True)
    back = back.reshape(groups * back_rows, LANES)
    count = token_count // members
    tail_width = model_width + LANES
    part = shape((count + SUBLANES, tail_width), I16)
    mine, to_right, to_left, to_across = call(
        lambda *refs: combine_kernel(members, groups, *refs),
        (part,) * 4,
        (member, back, pick),
        scalars=1,
        scratch=[VMEM((token_count, tail_width), F32), VMEM((groups * back_rows, LANES), F32)],
    )
    pieces = (
        lax.ppermute(to_right, "tp", right),
        lax.ppermute(to_left, "tp", left),
        lax.ppermute(to_across, "tp", across),
    )
    summed, gates_grad = call(
        sum_kernel,
        (shape((count, model_width), BF16), shape((top_count, token_count), F32)),
        (mine, *pieces, gate_weights.T),
    )
    pieces = (
        lax.ppermute(summed, "tp", right),
        lax.ppermute(summed, "tp", left),
        lax.ppermute(summed, "tp", across),
    )
    tokens_grad = call(
        lambda *refs: place_kernel(members, *refs),
        shape((token_count, model_width), BF16),
        (member, summed, *pieces),
        scalars=1,
    )

    sums = (
        shape((local_experts, model_width, hidden_width), F32),
        shape((local_experts, model_width, hidden_width), F32),
        shape((local_experts, hidden_width, model_width), F32),
    )

    def weight_sums(sources, earlier):
        count = sum(source.shape[0] for source in sources) // chunk * quarter
        return call(
            lambda *refs: weight_kernel(local_experts, quarter, len(sources), len(earlier), *refs),
            sums,
            (*sources, gate_proj, up_proj, down_proj, *earlier),
            scratch=[VMEM((count, model_width), BF16)] * 2,
        )

    near = weight_sums((landed, right_low, left_high), ())
    mid = weight_sums((right_high, left_low), near)
    gate_grad, up_grad, down_grad = weight_sums((opposite_low, opposite_high), mid)
    return (tokens_grad, gates_grad.T, gate_grad, up_grad, down_grad)


def solution(mesh):
    in_specs = (
        P("ep", None),
        P("ep", None),
        P("ep", None),
        P("ep", None),
        P("ep", None, "tp"),
        P("ep", None, "tp"),
        P("ep", "tp", None),
    )
    out_specs = (
        P("ep", None),
        P("ep", None),
        P("ep", None, "tp"),
        P("ep", None, "tp"),
        P("ep", "tp", None),
    )
    return jax.shard_map(step, mesh=mesh, in_specs=in_specs, out_specs=out_specs, check_vma=False)
```

```python
import jax
import jax.numpy as jnp
from jax import lax
from jax.experimental import pallas as pl
from jax.experimental.pallas import tpu as pltpu
from jax.sharding import PartitionSpec as P


F32 = jnp.float32
I16 = jnp.int16
BF16 = jnp.bfloat16
I32 = jnp.int32
LANES = 128
SUBLANES = 8
BLOCK = 16
HALVES = 2
TOP_CODE = 32766.0
STEPS = 8192.0
FINE = 32768.0
VMEM = pltpu.VMEM
SMEM = pltpu.SMEM
NN = ((1,), (0,))
NT = ((1,), (1,))
TN = ((0,), (0,))


def mm(a, b, dims=NN):
    return lax.dot_general(a, b, (dims, ((), ())), preferred_element_type=F32)


def iota(shape, dim):
    return lax.broadcasted_iota(I32, shape, dim)


def split3(value):
    high = value.astype(BF16)
    rest = value - high.astype(F32)
    middle = rest.astype(BF16)
    low = (rest - middle.astype(F32)).astype(BF16)
    return high, middle, low


def exponent(value):
    return jnp.floor(jnp.log(jnp.maximum(value, 1e-30)) * 1.4426950408889634)


def row_scale(power, steps):
    return steps * jnp.exp2(power) * (1.0 / (STEPS * TOP_CODE))


def code_rows(value):
    largest = jnp.maximum(jnp.max(jnp.abs(value), axis=1, keepdims=True), 1e-30)
    power = exponent(largest)
    steps = jnp.ceil(largest * jnp.exp2(-power) * STEPS)
    return jnp.round(value * (1.0 / row_scale(power, steps))), power, steps


def code_values(value):
    power = exponent(jnp.abs(value))
    value = value * jnp.exp2(-power) * STEPS
    coarse = jnp.round(value)
    return power, coarse, jnp.round((value - coarse) * FINE)


def decode_values(power, coarse, fine):
    return (coarse + fine * (1.0 / FINE)) * (jnp.exp2(power) * (1.0 / STEPS))


def to_code(value):
    return value.astype(I32).astype(I16)


def from_code(value):
    return value.astype(I32).astype(F32)


def dispatch_kernel(
    experts, local_experts, quarter, member, routing, weights, tokens, cotangent, rows_out, pick, laid
):
    token_count, _ = tokens.shape
    slots = pick.shape[1]
    group = local_experts * quarter
    devices = experts // local_experts
    expert = iota((experts, token_count), 0)
    chosen = [routing[k : k + 1, :] for k in range(2)]
    onehot = [jnp.where(expert == c, 1.0, 0.0) for c in chosen]
    earlier = iota((token_count, token_count), 0)
    later = iota((token_count, token_count), 1)
    upper = jnp.where(earlier < later, 1.0, 0.0).astype(BF16)
    before = mm((onehot[0] + onehot[1]).astype(BF16), upper)
    slot = iota((slots, token_count), 0)
    hits = []
    for k in range(2):
        position = jnp.sum(onehot[k] * before, axis=0, keepdims=True).astype(I32)
        local = position - member[0] * quarter
        present = (local >= 0) & (local < quarter)
        device = chosen[k] // local_experts
        within = (chosen[k] - device * local_experts) * quarter + local
        hits.append(slot == jnp.where(present, within * devices + device, -1))
        pick[k] = jnp.where(hits[k], 1.0, 0.0).astype(BF16)
    weighted = jnp.where(hits[0], weights[0:1, :], jnp.where(hits[1], weights[1:2, :], 0.0))
    slot_weight = jnp.sum(weighted, axis=1, keepdims=True)
    both = jnp.where(hits[0] | hits[1], 1.0, 0.0).astype(BF16)
    values = (mm(both, tokens[...]), mm(both, cotangent[...]) * slot_weight)
    tiles = laid.shape[0]
    chunk = HALVES * 2 * group
    for kind, value in enumerate(values):
        for h in range(HALVES):
            for at in range(group):
                to = (2 * h + kind) * group + at
                for tile in range(tiles):
                    column = (h * tiles + tile) * LANES
                    piece = value[at * devices : (at + 1) * devices, column : column + LANES]
                    laid[tile, pl.ds(to, devices, stride=chunk), :] = piece
    for tile in range(tiles):
        rows_out[:, tile * LANES : (tile + 1) * LANES] = laid[tile].astype(BF16)


def land(source, expert, local_experts, quarter, rows, scaled, offset):
    half = source.shape[1]
    group = local_experts * quarter
    chunk = HALVES * 2 * group
    out_rows = BLOCK * quarter
    index = iota((HALVES * 2 * out_rows, 1), 0)
    kind = index // out_rows
    rest = index - kind * out_rows
    slot = rest // BLOCK
    wanted = (rest - slot * BLOCK) * chunk + kind * group + expert * quarter + slot
    column = iota((HALVES * 2 * out_rows, BLOCK * chunk), 1)
    permutation = jnp.where(column == wanted, 1.0, 0.0).astype(BF16)
    for block in range(source.shape[0] // (BLOCK * chunk)):
        moved = mm(permutation, source[block * BLOCK * chunk : (block + 1) * BLOCK * chunk, :])
        moved = moved.astype(BF16)
        at = slice(offset + block * out_rows, offset + (block + 1) * out_rows)
        for h in range(HALVES):
            columns = slice(h * half, (h + 1) * half)
            first = 2 * h * out_rows
            rows[at, columns] = moved[first : first + out_rows]
            scaled[at, columns] = moved[first + out_rows : first + 2 * out_rows]


def hidden_terms(gate_pre, up_pre, hidden_grad):
    gate_pre = gate_pre.astype(BF16).astype(F32)
    up_pre = up_pre.astype(BF16).astype(F32)
    sigmoid = jax.nn.sigmoid(gate_pre)
    activated = gate_pre * sigmoid
    hidden = activated * up_pre
    gate_grad = (hidden_grad * up_pre * sigmoid * (1.0 + gate_pre * (1.0 - sigmoid))).astype(BF16)
    up_grad = (hidden_grad * activated).astype(BF16)
    return hidden, gate_grad, up_grad


def input_kernel(local_experts, quarter, landed, *refs):
    gates, ups, downs = refs[0:4], refs[4:8], refs[8:11]
    down_even, down_odd, out, rows, scaled, coded = refs[11:]
    own, _ = rows.shape
    slots = local_experts * quarter
    devices = own // quarter
    stride = (slots + 1) * SUBLANES
    expert = pl.program_id(0)

    @pl.when(expert == 0)
    def _():
        for i in range(slots, SUBLANES):
            at = slots * SUBLANES + i
            coded[pl.ds(at, devices, stride=stride), :] = jnp.zeros((devices, LANES), F32)

    land(landed, expert, local_experts, quarter, rows, scaled, 0)
    gate = jnp.concatenate([g[0] for g in gates], axis=1)
    up = jnp.concatenate([u[0] for u in ups], axis=1)
    last = jnp.where(expert == 0, down_even[0], down_odd[0])
    down = jnp.concatenate([d[0] for d in downs] + [last], axis=0)
    hidden_grad = mm(scaled[...], down, NT)
    hidden, gate_grad, up_grad = hidden_terms(mm(rows[...], gate), mm(rows[...], up), hidden_grad)
    product = jnp.sum(hidden_grad * hidden, axis=1, keepdims=True)
    grad = mm(gate_grad, gate, NT) + mm(up_grad, up, NT)
    grad, power, steps = code_rows(grad)
    lane = iota((own, LANES), 1)
    tail = jnp.zeros((own, LANES), F32)
    for at, column in enumerate((power, steps) + code_values(product)):
        tail = jnp.where(lane == at, column, tail)
    for block in range(devices // BLOCK):
        for q in range(quarter):
            at = (block * quarter + q) * BLOCK
            to = block * BLOCK * stride
            slot = expert * quarter + q
            for i in range(SUBLANES):
                piece = grad[at : at + BLOCK, i * LANES : (i + 1) * LANES]
                coded[pl.ds(to + slot * SUBLANES + i, BLOCK, stride=stride), :] = piece
            to += slots * SUBLANES + slot
            coded[pl.ds(to, BLOCK, stride=stride), :] = tail[at : at + BLOCK]

    @pl.when(expert == local_experts - 1)
    def _():
        out[...] = to_code(coded[...])


def weight_kernel(local_experts, quarter, source_count, earlier_count, *refs):
    sources, refs = refs[:source_count], refs[source_count:]
    (gate, up, down), refs = refs[:3], refs[3:]
    earlier, refs = refs[:earlier_count], refs[earlier_count:]
    outs, (rows, scaled) = refs[:3], refs[3:]
    chunk = HALVES * 2 * local_experts * quarter
    hidden_width = gate.shape[2]

    expert = pl.program_id(0)
    offset = 0
    for source in sources:
        land(source, expert, local_experts, quarter, rows, scaled, offset)
        offset += source.shape[0] // chunk * quarter
    both = mm(rows[...], jnp.concatenate([gate[0], up[0]], axis=1))
    hidden_grad = mm(scaled[...], down[0], NT)
    hidden, gate_grad, up_grad = hidden_terms(
        both[:, :hidden_width], both[:, hidden_width:], hidden_grad
    )
    grads = mm(rows[...], jnp.concatenate([gate_grad, up_grad], axis=1), TN)
    down_grad = mm(hidden.astype(BF16), scaled[...], TN)
    for at, part in enumerate((grads[:, :hidden_width], grads[:, hidden_width:], down_grad)):
        outs[at][0] = earlier[at][0] + part if earlier else part


def member_rows(member, distance, members, count):
    return pl.ds(pl.multiple_of(lax.rem(member + distance, members) * count, count), count)


def combine_kernel(members, devices, member, coded, pick, *refs):
    outs, total, back = refs[:-2], refs[-2], refs[-1]
    back[...] = from_code(coded[...])
    token_count, tail_width = total.shape
    width = tail_width - LANES
    slots = pick.shape[1] // devices
    stride = (slots + 1) * SUBLANES
    tails = [
        back[pl.ds(slots * SUBLANES + slot, devices, stride=stride), :] for slot in range(slots)
    ]
    tail = jnp.concatenate(tails, axis=0)
    scale = row_scale(tail[:, 0:1], tail[:, 1:2])
    columns = []
    for i in range(SUBLANES):
        pieces = [
            back[pl.ds(slot * SUBLANES + i, devices, stride=stride), :] for slot in range(slots)
        ]
        columns.append(jnp.concatenate(pieces, axis=0))
    grad = jnp.concatenate(columns, axis=1) * scale
    both = pick[0] + pick[1]
    grad, power, steps = code_rows(sum(mm(both, part, TN) for part in split3(grad)[:2]))
    total[:, 0:width] = grad
    lane = iota((token_count, LANES), 1)
    total[:, width:] = jnp.where(lane == 0, power, jnp.where(lane == 1, steps, 0.0))
    product = decode_values(tail[:, 2:3], tail[:, 3:4], tail[:, 4:5])
    sums = [jnp.sum(pick[k].astype(F32) * product, axis=0, keepdims=True) for k in range(2)]
    power, coarse, fine = code_values(jnp.concatenate(sums, axis=1))
    spare = jnp.zeros((1, tail_width - 4 * token_count), F32)
    first = jnp.concatenate([power, coarse, spare], axis=1)
    second = jnp.concatenate([fine, jnp.zeros_like(fine), spare], axis=1)
    line = iota((SUBLANES, tail_width), 0)
    lines = to_code(jnp.where(line == 0, first, jnp.where(line == 1, second, 0.0)))
    count = token_count // members
    for out, distance in zip(outs, (0, 1, 3, 2)):
        out[0:count, :] = to_code(total[member_rows(member[0], distance, members, count), :])
        out[count : count + SUBLANES, :] = lines


def sum_kernel(own, from_left, from_right, from_opposite, weights, grad_out, gates_out):
    count, width = grad_out.shape
    token_count = weights.shape[1]
    parts = [from_code(part[...]) for part in (own, from_left, from_right, from_opposite)]
    grads = [
        part[:count, :width] * row_scale(part[:count, width : width + 1], part[:count, width + 1 : width + 2])
        for part in parts
    ]
    grad_out[...] = ((grads[0] + grads[3]) + (grads[1] + grads[2])).astype(BF16)
    values = 2 * token_count
    products = [
        decode_values(
            part[count : count + 1, 0:values],
            part[count : count + 1, values : 2 * values],
            part[count + 1 : count + 2, 0:values],
        )
        for part in parts
    ]
    product = (products[0] + products[3]) + (products[1] + products[2])
    for k in range(2):
        gates_out[k : k + 1, :] = product[:, k * token_count : (k + 1) * token_count] / weights[k : k + 1, :]


def step(tokens, cotangent, routing, gate_weights, gate_proj, up_proj, down_proj):
    token_count, model_width = tokens.shape
    top_count = routing.shape[1]
    local_experts, _, hidden_width = gate_proj.shape
    groups = lax.axis_size("ep")
    members = lax.axis_size("tp")
    experts = local_experts * groups
    capacity = members * (
        (3 * token_count * top_count + experts * members - 1) // (experts * members)
    )
    quarter = capacity // members
    slots = experts * quarter
    own = groups * quarter
    chunk = HALVES * 2 * local_experts * quarter
    half = model_width // HALVES
    member = lax.axis_index("tp").astype(I32).reshape(1)
    right = [(i, (i + 1) % members) for i in range(members)]
    left = [(i, (i - 1) % members) for i in range(members)]
    across = [(i, (i + 2) % members) for i in range(members)]
    whole = pl.BlockSpec(memory_space=VMEM)
    scalar = pl.BlockSpec(memory_space=SMEM)

    def per_expert(array):
        return pl.BlockSpec((1,) + array.shape[1:], lambda e: (e, 0, 0))

    def constant(array):
        return pl.BlockSpec(array.shape, lambda e: (0,) * len(array.shape))

    def call(kernel, out_shape, args, scalars=0, scratch=(), specs=None):
        in_specs = [scalar] * scalars + [whole] * (len(args) - scalars)
        return pl.pallas_call(
            kernel,
            grid=(local_experts,) if specs else (),
            out_shape=out_shape,
            in_specs=specs[0] if specs else in_specs,
            out_specs=specs[1] if specs else jax.tree.map(lambda _: whole, out_shape),
            scratch_shapes=list(scratch),
        )(*args)

    def shape(dims, dtype):
        return jax.ShapeDtypeStruct(dims, dtype)

    gates, ups, downs = [gate_proj], [up_proj], [down_proj]
    for kept, mine in ((gates, gate_proj), (ups, up_proj), (downs, down_proj)):
        kept.append(lax.ppermute(mine, "tp", right))
        kept.append(lax.ppermute(mine, "tp", left))
    gates.append(lax.ppermute(gates[2], "tp", left))
    ups.append(lax.ppermute(ups[1], "tp", right))
    down_even = lax.ppermute(downs[2][0:1], "tp", left)
    down_odd = lax.ppermute(downs[1][1:2], "tp", right)

    send, pick = call(
        lambda *refs: dispatch_kernel(experts, local_experts, quarter, *refs),
        (shape((groups * chunk, half), BF16), shape((2, slots, token_count), BF16)),
        (member, routing.T, gate_weights.T, tokens, cotangent),
        scalars=1,
        scratch=[VMEM((half // LANES, groups * chunk, LANES), F32)],
    )
    landed = lax.all_to_all(
        send.reshape(groups, chunk, half), "ep", split_axis=0, concat_axis=0, tiled=True
    ).reshape(groups * chunk, half)

    middle = groups * chunk // 2
    low, high = landed[:middle], landed[middle:]
    left_high = lax.ppermute(high, "tp", right)
    right_low = lax.ppermute(low, "tp", left)
    right_high = lax.ppermute(high, "tp", left)
    left_low = lax.ppermute(low, "tp", right)
    opposite_low = lax.ppermute(right_low, "tp", left)
    opposite_high = lax.ppermute(left_high, "tp", right)

    back_rows = (local_experts * quarter + 1) * SUBLANES
    back = call(
        lambda *refs: input_kernel(local_experts, quarter, *refs),
        shape((groups * back_rows, LANES), I16),
        (landed, *gates, *ups, *downs, down_even, down_odd),
        scratch=[VMEM((own, model_width), BF16)] * 2 + [VMEM((groups * back_rows, LANES), F32)],
        specs=(
            [constant(landed)]
            + [per_expert(a) for a in (*gates, *ups, *downs)]
            + [constant(down_even), constant(down_odd)],
            pl.BlockSpec((groups * back_rows, LANES), lambda e: (0, 0)),
        ),
    )
    back = back.reshape(groups, back_rows, LANES)
    back = lax.all_to_all(back, "ep", split_axis=0, concat_axis=0, tiled=True)
    back = back.reshape(groups * back_rows, LANES)
    count = token_count // members
    tail_width = model_width + LANES
    part = shape((count + SUBLANES, tail_width), I16)
    mine, to_right, to_left, to_across = call(
        lambda *refs: combine_kernel(members, groups, *refs),
        (part,) * 4,
        (member, back, pick),
        scalars=1,
        scratch=[VMEM((token_count, tail_width), F32), VMEM((groups * back_rows, LANES), F32)],
    )
    pieces = (
        lax.ppermute(to_right, "tp", right),
        lax.ppermute(to_left, "tp", left),
        lax.ppermute(to_across, "tp", across),
    )
    summed, gates_grad = call(
        sum_kernel,
        (shape((count, model_width), BF16), shape((top_count, token_count), F32)),
        (mine, *pieces, gate_weights.T),
    )
    pieces = (
        lax.ppermute(summed, "tp", right),
        lax.ppermute(summed, "tp", left),
        lax.ppermute(summed, "tp", across),
    )
    tokens_grad = jnp.zeros((token_count, model_width), BF16)
    from_left_sum, from_right_sum, from_across_sum = pieces
    placed = ((summed, 0), (from_left_sum, 3), (from_right_sum, 1), (from_across_sum, 2))
    for piece, distance in placed:
        at = lax.rem(member[0] + distance, members) * count
        tokens_grad = lax.dynamic_update_slice(tokens_grad, piece, (at, 0))

    sums = (
        shape((local_experts, model_width, hidden_width), F32),
        shape((local_experts, model_width, hidden_width), F32),
        shape((local_experts, hidden_width, model_width), F32),
    )

    def weight_sums(sources, earlier):
        count = sum(source.shape[0] for source in sources) // chunk * quarter
        shared = (gate_proj, up_proj, down_proj, *earlier)
        return call(
            lambda *refs: weight_kernel(local_experts, quarter, len(sources), len(earlier), *refs),
            sums,
            (*sources, *shared),
            scratch=[VMEM((count, model_width), BF16)] * 2,
            specs=(
                [constant(a) for a in sources] + [per_expert(a) for a in shared],
                tuple(per_expert(a) for a in sums),
            ),
        )

    near = weight_sums((landed, right_low, left_high), ())
    mid = weight_sums((right_high, left_low), near)
    gate_grad, up_grad, down_grad = weight_sums((opposite_low, opposite_high), mid)
    return (tokens_grad, gates_grad.T, gate_grad, up_grad, down_grad)


def solution(mesh):
    in_specs = (
        P("ep", None),
        P("ep", None),
        P("ep", None),
        P("ep", None),
        P("ep", None, "tp"),
        P("ep", None, "tp"),
        P("ep", "tp", None),
    )
    out_specs = (
        P("ep", None),
        P("ep", None),
        P("ep", None, "tp"),
        P("ep", None, "tp"),
        P("ep", "tp", None),
    )
    return jax.shard_map(step, mesh=mesh, in_specs=in_specs, out_specs=out_specs, check_vma=False)
```

```python
import jax
import jax.numpy as jnp
from jax import lax
from jax.experimental import pallas as pl
from jax.experimental.pallas import tpu as pltpu
from jax.sharding import PartitionSpec as P


F32 = jnp.float32
I16 = jnp.int16
BF16 = jnp.bfloat16
I32 = jnp.int32
LANES = 128
SUBLANES = 8
BLOCK = 16
HALVES = 2
TOP_CODE = 32766.0
STEPS = 8192.0
FINE = 32768.0
VMEM = pltpu.VMEM
SMEM = pltpu.SMEM
NN = ((1,), (0,))
NT = ((1,), (1,))
TN = ((0,), (0,))


def mm(a, b, dims=NN):
    return lax.dot_general(a, b, (dims, ((), ())), preferred_element_type=F32)


def iota(shape, dim):
    return lax.broadcasted_iota(I32, shape, dim)


def split3(value):
    high = value.astype(BF16)
    rest = value - high.astype(F32)
    middle = rest.astype(BF16)
    low = (rest - middle.astype(F32)).astype(BF16)
    return high, middle, low


def exponent(value):
    return jnp.floor(jnp.log(jnp.maximum(value, 1e-30)) * 1.4426950408889634)


def row_scale(power, steps):
    return steps * jnp.exp2(power) * (1.0 / (STEPS * TOP_CODE))


def code_rows(value):
    largest = jnp.maximum(jnp.max(jnp.abs(value), axis=1, keepdims=True), 1e-30)
    power = exponent(largest)
    steps = jnp.ceil(largest * jnp.exp2(-power) * STEPS)
    return jnp.round(value * (1.0 / row_scale(power, steps))), power, steps


def code_values(value):
    power = exponent(jnp.abs(value))
    value = value * jnp.exp2(-power) * STEPS
    coarse = jnp.round(value)
    return power, coarse, jnp.round((value - coarse) * FINE)


def decode_values(power, coarse, fine):
    return (coarse + fine * (1.0 / FINE)) * (jnp.exp2(power) * (1.0 / STEPS))


def to_code(value):
    return value.astype(I32).astype(I16)


def from_code(value):
    return value.astype(I32).astype(F32)


def dispatch_kernel(
    experts, local_experts, quarter, member, routing, weights, tokens, cotangent, rows_out, pick, laid
):
    token_count, _ = tokens.shape
    slots = pick.shape[1]
    group = local_experts * quarter
    devices = experts // local_experts
    expert = iota((experts, token_count), 0)
    chosen = [routing[k : k + 1, :] for k in range(2)]
    onehot = [jnp.where(expert == c, 1.0, 0.0) for c in chosen]
    earlier = iota((token_count, token_count), 0)
    later = iota((token_count, token_count), 1)
    upper = jnp.where(earlier < later, 1.0, 0.0).astype(BF16)
    before = mm((onehot[0] + onehot[1]).astype(BF16), upper)
    slot = iota((slots, token_count), 0)
    hits = []
    for k in range(2):
        position = jnp.sum(onehot[k] * before, axis=0, keepdims=True).astype(I32)
        local = position - member[0] * quarter
        present = (local >= 0) & (local < quarter)
        device = chosen[k] // local_experts
        within = (chosen[k] - device * local_experts) * quarter + local
        hits.append(slot == jnp.where(present, within * devices + device, -1))
        pick[k] = jnp.where(hits[k], 1.0, 0.0).astype(BF16)
    weighted = jnp.where(hits[0], weights[0:1, :], jnp.where(hits[1], weights[1:2, :], 0.0))
    slot_weight = jnp.sum(weighted, axis=1, keepdims=True)
    both = jnp.where(hits[0] | hits[1], 1.0, 0.0).astype(BF16)
    values = (mm(both, tokens[...]), mm(both, cotangent[...]) * slot_weight)
    tiles = laid.shape[0]
    chunk = HALVES * 2 * group
    for kind, value in enumerate(values):
        for h in range(HALVES):
            for at in range(group):
                to = (2 * h + kind) * group + at
                for tile in range(tiles):
                    column = (h * tiles + tile) * LANES
                    piece = value[at * devices : (at + 1) * devices, column : column + LANES]
                    laid[tile, pl.ds(to, devices, stride=chunk), :] = piece
    for tile in range(tiles):
        rows_out[:, tile * LANES : (tile + 1) * LANES] = laid[tile].astype(BF16)


def land(source, expert, local_experts, quarter, rows, scaled, offset):
    half = source.shape[1]
    group = local_experts * quarter
    chunk = HALVES * 2 * group
    out_rows = BLOCK * quarter
    index = iota((HALVES * 2 * out_rows, 1), 0)
    kind = index // out_rows
    rest = index - kind * out_rows
    slot = rest // BLOCK
    wanted = (rest - slot * BLOCK) * chunk + kind * group + expert * quarter + slot
    column = iota((HALVES * 2 * out_rows, BLOCK * chunk), 1)
    permutation = jnp.where(column == wanted, 1.0, 0.0).astype(BF16)
    for block in range(source.shape[0] // (BLOCK * chunk)):
        moved = mm(permutation, source[block * BLOCK * chunk : (block + 1) * BLOCK * chunk, :])
        moved = moved.astype(BF16)
        at = slice(offset + block * out_rows, offset + (block + 1) * out_rows)
        for h in range(HALVES):
            columns = slice(h * half, (h + 1) * half)
            first = 2 * h * out_rows
            rows[at, columns] = moved[first : first + out_rows]
            scaled[at, columns] = moved[first + out_rows : first + 2 * out_rows]


def hidden_terms(gate_pre, up_pre, hidden_grad):
    gate_pre = gate_pre.astype(BF16).astype(F32)
    up_pre = up_pre.astype(BF16).astype(F32)
    sigmoid = jax.nn.sigmoid(gate_pre)
    activated = gate_pre * sigmoid
    hidden = activated * up_pre
    gate_grad = (hidden_grad * up_pre * sigmoid * (1.0 + gate_pre * (1.0 - sigmoid))).astype(BF16)
    up_grad = (hidden_grad * activated).astype(BF16)
    return hidden, gate_grad, up_grad


def input_kernel(local_experts, quarter, landed, *refs):
    gates, ups, downs = refs[0:4], refs[4:8], refs[8:11]
    down_even, down_odd, out, rows, scaled, coded = refs[11:]
    own, _ = rows.shape
    slots = local_experts * quarter
    devices = own // quarter
    stride = (slots + 1) * SUBLANES
    expert = pl.program_id(0)

    @pl.when(expert == 0)
    def _():
        for i in range(slots, SUBLANES):
            at = slots * SUBLANES + i
            coded[pl.ds(at, devices, stride=stride), :] = jnp.zeros((devices, LANES), F32)

    land(landed, expert, local_experts, quarter, rows, scaled, 0)
    gate = jnp.concatenate([g[0] for g in gates], axis=1)
    up = jnp.concatenate([u[0] for u in ups], axis=1)
    last = jnp.where(expert == 0, down_even[0], down_odd[0])
    down = jnp.concatenate([d[0] for d in downs] + [last], axis=0)
    hidden_grad = mm(scaled[...], down, NT)
    hidden, gate_grad, up_grad = hidden_terms(mm(rows[...], gate), mm(rows[...], up), hidden_grad)
    product = jnp.sum(hidden_grad * hidden, axis=1, keepdims=True)
    grad = mm(gate_grad, gate, NT) + mm(up_grad, up, NT)
    grad, power, steps = code_rows(grad)
    lane = iota((own, LANES), 1)
    tail = jnp.zeros((own, LANES), F32)
    for at, column in enumerate((power, steps) + code_values(product)):
        tail = jnp.where(lane == at, column, tail)
    for block in range(devices // BLOCK):
        for q in range(quarter):
            at = (block * quarter + q) * BLOCK
            to = block * BLOCK * stride
            slot = expert * quarter + q
            for i in range(SUBLANES):
                piece = grad[at : at + BLOCK, i * LANES : (i + 1) * LANES]
                coded[pl.ds(to + slot * SUBLANES + i, BLOCK, stride=stride), :] = piece
            to += slots * SUBLANES + slot
            coded[pl.ds(to, BLOCK, stride=stride), :] = tail[at : at + BLOCK]

    @pl.when(expert == local_experts - 1)
    def _():
        out[...] = to_code(coded[...])


def weight_kernel(local_experts, quarter, source_count, earlier_count, *refs):
    sources, refs = refs[:source_count], refs[source_count:]
    (gate, up, down), refs = refs[:3], refs[3:]
    earlier, refs = refs[:earlier_count], refs[earlier_count:]
    outs, (rows, scaled) = refs[:3], refs[3:]
    chunk = HALVES * 2 * local_experts * quarter
    hidden_width = gate.shape[2]

    expert = pl.program_id(0)
    offset = 0
    for source in sources:
        land(source, expert, local_experts, quarter, rows, scaled, offset)
        offset += source.shape[0] // chunk * quarter
    both = mm(rows[...], jnp.concatenate([gate[0], up[0]], axis=1))
    hidden_grad = mm(scaled[...], down[0], NT)
    hidden, gate_grad, up_grad = hidden_terms(
        both[:, :hidden_width], both[:, hidden_width:], hidden_grad
    )
    grads = mm(rows[...], jnp.concatenate([gate_grad, up_grad], axis=1), TN)
    down_grad = mm(hidden.astype(BF16), scaled[...], TN)
    for at, part in enumerate((grads[:, :hidden_width], grads[:, hidden_width:], down_grad)):
        outs[at][0] = earlier[at][0] + part if earlier else part


def member_rows(member, distance, members, count):
    return pl.ds(pl.multiple_of(lax.rem(member + distance, members) * count, count), count)


def combine_kernel(members, devices, member, coded, pick, *refs):
    outs, total, back = refs[:-2], refs[-2], refs[-1]
    back[...] = from_code(coded[...])
    token_count, tail_width = total.shape
    width = tail_width - LANES
    slots = pick.shape[1] // devices
    stride = (slots + 1) * SUBLANES
    tails = [
        back[pl.ds(slots * SUBLANES + slot, devices, stride=stride), :] for slot in range(slots)
    ]
    tail = jnp.concatenate(tails, axis=0)
    scale = row_scale(tail[:, 0:1], tail[:, 1:2])
    columns = []
    for i in range(SUBLANES):
        pieces = [
            back[pl.ds(slot * SUBLANES + i, devices, stride=stride), :] for slot in range(slots)
        ]
        columns.append(jnp.concatenate(pieces, axis=0))
    grad = jnp.concatenate(columns, axis=1) * scale
    both = pick[0] + pick[1]
    grad, power, steps = code_rows(sum(mm(both, part, TN) for part in split3(grad)[:2]))
    total[:, 0:width] = grad
    lane = iota((token_count, LANES), 1)
    total[:, width:] = jnp.where(lane == 0, power, jnp.where(lane == 1, steps, 0.0))
    product = decode_values(tail[:, 2:3], tail[:, 3:4], tail[:, 4:5])
    sums = [jnp.sum(pick[k].astype(F32) * product, axis=0, keepdims=True) for k in range(2)]
    power, coarse, fine = code_values(jnp.concatenate(sums, axis=1))
    spare = jnp.zeros((1, tail_width - 4 * token_count), F32)
    first = jnp.concatenate([power, coarse, spare], axis=1)
    second = jnp.concatenate([fine, jnp.zeros_like(fine), spare], axis=1)
    line = iota((SUBLANES, tail_width), 0)
    lines = to_code(jnp.where(line == 0, first, jnp.where(line == 1, second, 0.0)))
    count = token_count // members
    for out, distance in zip(outs, (0, 1, 3, 2)):
        out[0:count, :] = to_code(total[member_rows(member[0], distance, members, count), :])
        out[count : count + SUBLANES, :] = lines


def sum_kernel(own, from_left, from_right, from_opposite, weights, grad_out, gates_out):
    count, width = grad_out.shape
    token_count = weights.shape[1]
    parts = [from_code(part[...]) for part in (own, from_left, from_right, from_opposite)]
    grads = [
        part[:count, :width] * row_scale(part[:count, width : width + 1], part[:count, width + 1 : width + 2])
        for part in parts
    ]
    grad_out[...] = ((grads[0] + grads[3]) + (grads[1] + grads[2])).astype(BF16)
    values = 2 * token_count
    products = [
        decode_values(
            part[count : count + 1, 0:values],
            part[count : count + 1, values : 2 * values],
            part[count + 1 : count + 2, 0:values],
        )
        for part in parts
    ]
    product = (products[0] + products[3]) + (products[1] + products[2])
    for k in range(2):
        gates_out[k : k + 1, :] = product[:, k * token_count : (k + 1) * token_count] / weights[k : k + 1, :]


def step(tokens, cotangent, routing, gate_weights, gate_proj, up_proj, down_proj):
    token_count, model_width = tokens.shape
    top_count = routing.shape[1]
    local_experts, _, hidden_width = gate_proj.shape
    groups = lax.axis_size("ep")
    members = lax.axis_size("tp")
    experts = local_experts * groups
    capacity = members * (
        (3 * token_count * top_count + experts * members - 1) // (experts * members)
    )
    quarter = capacity // members
    slots = experts * quarter
    own = groups * quarter
    chunk = HALVES * 2 * local_experts * quarter
    half = model_width // HALVES
    member = lax.axis_index("tp").astype(I32).reshape(1)
    right = [(i, (i + 1) % members) for i in range(members)]
    left = [(i, (i - 1) % members) for i in range(members)]
    across = [(i, (i + 2) % members) for i in range(members)]
    whole = pl.BlockSpec(memory_space=VMEM)
    scalar = pl.BlockSpec(memory_space=SMEM)

    def per_expert(array):
        return pl.BlockSpec((1,) + array.shape[1:], lambda e: (e, 0, 0))

    def constant(array):
        return pl.BlockSpec(array.shape, lambda e: (0,) * len(array.shape))

    def call(kernel, out_shape, args, scalars=0, scratch=(), specs=None):
        in_specs = [scalar] * scalars + [whole] * (len(args) - scalars)
        return pl.pallas_call(
            kernel,
            grid=(local_experts,) if specs else (),
            out_shape=out_shape,
            in_specs=specs[0] if specs else in_specs,
            out_specs=specs[1] if specs else jax.tree.map(lambda _: whole, out_shape),
            scratch_shapes=list(scratch),
        )(*args)

    def shape(dims, dtype):
        return jax.ShapeDtypeStruct(dims, dtype)

    gates, ups, downs = [gate_proj], [up_proj], [down_proj]
    for kept, mine in ((gates, gate_proj), (ups, up_proj), (downs, down_proj)):
        kept.append(lax.ppermute(mine, "tp", right))
        kept.append(lax.ppermute(mine, "tp", left))
    gates.append(lax.ppermute(gates[2], "tp", left))
    ups.append(lax.ppermute(ups[1], "tp", right))
    down_even = lax.ppermute(downs[2][0:1], "tp", left)
    down_odd = lax.ppermute(downs[1][1:2], "tp", right)

    send, pick = call(
        lambda *refs: dispatch_kernel(experts, local_experts, quarter, *refs),
        (shape((groups * chunk, half), BF16), shape((2, slots, token_count), BF16)),
        (member, routing.T, gate_weights.T, tokens, cotangent),
        scalars=1,
        scratch=[VMEM((half // LANES, groups * chunk, LANES), F32)],
    )
    landed = lax.all_to_all(
        send.reshape(groups, chunk, half), "ep", split_axis=0, concat_axis=0, tiled=True
    ).reshape(groups * chunk, half)

    middle = groups * chunk // 2
    low, high = landed[:middle], landed[middle:]
    left_high = lax.ppermute(high, "tp", right)
    right_low = lax.ppermute(low, "tp", left)
    right_high = lax.ppermute(high, "tp", left)
    left_low = lax.ppermute(low, "tp", right)
    opposite_low = lax.ppermute(right_low, "tp", left)
    opposite_high = lax.ppermute(left_high, "tp", right)

    back_rows = (local_experts * quarter + 1) * SUBLANES
    back = call(
        lambda *refs: input_kernel(local_experts, quarter, *refs),
        shape((groups * back_rows, LANES), I16),
        (landed, *gates, *ups, *downs, down_even, down_odd),
        scratch=[VMEM((own, model_width), BF16)] * 2 + [VMEM((groups * back_rows, LANES), F32)],
        specs=(
            [constant(landed)]
            + [per_expert(a) for a in (*gates, *ups, *downs)]
            + [constant(down_even), constant(down_odd)],
            pl.BlockSpec((groups * back_rows, LANES), lambda e: (0, 0)),
        ),
    )
    back = back.reshape(groups, back_rows, LANES)
    back = lax.all_to_all(back, "ep", split_axis=0, concat_axis=0, tiled=True)
    back = back.reshape(groups * back_rows, LANES)
    count = token_count // members
    tail_width = model_width + LANES
    part = shape((count + SUBLANES, tail_width), I16)
    mine, to_right, to_left, to_across = call(
        lambda *refs: combine_kernel(members, groups, *refs),
        (part,) * 4,
        (member, back, pick),
        scalars=1,
        scratch=[VMEM((token_count, tail_width), F32), VMEM((groups * back_rows, LANES), F32)],
    )
    far_piece = lax.ppermute(to_across, "tp", across)
    pieces = (
        lax.ppermute(to_right, "tp", right),
        lax.ppermute(to_left, "tp", left),
        far_piece,
    )
    summed, gates_grad = call(
        sum_kernel,
        (shape((count, model_width), BF16), shape((top_count, token_count), F32)),
        (mine, *pieces, gate_weights.T),
    )
    far_piece = lax.ppermute(summed, "tp", across)
    pieces = (
        lax.ppermute(summed, "tp", right),
        lax.ppermute(summed, "tp", left),
        far_piece,
    )
    tokens_grad = jnp.zeros((token_count, model_width), BF16)
    from_left_sum, from_right_sum, from_across_sum = pieces
    placed = ((summed, 0), (from_left_sum, 3), (from_right_sum, 1), (from_across_sum, 2))
    for piece, distance in placed:
        at = lax.rem(member[0] + distance, members) * count
        tokens_grad = lax.dynamic_update_slice(tokens_grad, piece, (at, 0))

    sums = (
        shape((local_experts, model_width, hidden_width), F32),
        shape((local_experts, model_width, hidden_width), F32),
        shape((local_experts, hidden_width, model_width), F32),
    )

    def weight_sums(sources, earlier):
        count = sum(source.shape[0] for source in sources) // chunk * quarter
        shared = (gate_proj, up_proj, down_proj, *earlier)
        return call(
            lambda *refs: weight_kernel(local_experts, quarter, len(sources), len(earlier), *refs),
            sums,
            (*sources, *shared),
            scratch=[VMEM((count, model_width), BF16)] * 2,
            specs=(
                [constant(a) for a in sources] + [per_expert(a) for a in shared],
                tuple(per_expert(a) for a in sums),
            ),
        )

    near = weight_sums((landed, right_low, left_high), ())
    mid = weight_sums((right_high, left_low), near)
    gate_grad, up_grad, down_grad = weight_sums((opposite_low, opposite_high), mid)
    return (tokens_grad, gates_grad.T, gate_grad, up_grad, down_grad)


def solution(mesh):
    in_specs = (
        P("ep", None),
        P("ep", None),
        P("ep", None),
        P("ep", None),
        P("ep", None, "tp"),
        P("ep", None, "tp"),
        P("ep", "tp", None),
    )
    out_specs = (
        P("ep", None),
        P("ep", None),
        P("ep", None, "tp"),
        P("ep", None, "tp"),
        P("ep", "tp", None),
    )
    return jax.shard_map(step, mesh=mesh, in_specs=in_specs, out_specs=out_specs, check_vma=False)
```
